32 devices in a mesh: sp: 16 (over z, y, x), tp: 2 (over core).
Axes of the slice: x: 2, y: 2, z: 4, core: 2. Of those that a mesh axis runs over, the one named last changes fastest.
Arguments:
- hidden: bfloat16 [3072, 2048], P('sp')
- norm_gain: float32 [2048], replicated, may hold values from 0.1 to 1.9
- query_weight: bfloat16 [2048, 1024], P(None, 'tp'), may hold values from -0.125 to 0.125
- key_weight: bfloat16 [2048, 256], replicated, may hold values from -0.125 to 0.125
- value_weight: bfloat16 [2048, 256], replicated, may hold values from -0.125 to 0.125
- head_bias: float32 [16], P('tp'), may hold values from -10 to -3.5
- output_weight: bfloat16 [1024, 2048], P('tp'), may hold values from -0.1875 to 0.1875
Outputs:
- mixed: bfloat16 [3072, 2048], P('sp')
The draws below stay inside these ranges and needn't reach their ends.
All inputs are finite; a program needn't handle non-finite values.
Results may differ from the reference program's by a relative error of at most 0.014.
Values may be sent and summed in bfloat16 or wider, within the bound.
A program may use at most 64 MiB of HBM per device.

```python
import math
import jax
import jax.numpy as jnp
from jax import lax

D = 2048
HEADS = 16
KV_HEADS = 4
HEAD_DIM = 64
TOK_DEV = 192
TOKENS = 3072


def draw_hidden(key, part):
    noise_key = jax.random.fold_in(key, 11)
    shift_key = jax.random.fold_in(key, 12)
    block_count = TOKENS // TOK_DEV
    offsets = jax.random.normal(shift_key, (block_count, 1, D), jnp.float32) * 0.8
    noise = jax.random.normal(noise_key, (block_count, TOK_DEV, D), jnp.float32)
    full = noise + offsets
    return full.reshape(TOKENS, D).astype(jnp.bfloat16)


def draw_head_bias(key, part):
    order = jax.random.permutation(jax.random.fold_in(key, 21), HEADS)
    values_key = jax.random.fold_in(key, 22)
    quick = order < HEADS // 2
    slow_value = jax.random.uniform(values_key, (HEADS,), jnp.float32, -9.8, -9.0)
    quick_value = jax.random.uniform(jax.random.fold_in(key, 23), (HEADS,), jnp.float32, -4.3, -3.7)
    return jnp.where(quick, quick_value, slow_value)


def block_scale(stream_key, shape, pieces, least, top_value):
    loudness, own = 1.0, jax.random.fold_in(stream_key, 6)
    for position, shards_of in pieces:
        draws = jnp.exp(jax.random.uniform(jax.random.fold_in(own, position), (shards_of,), jnp.float32, least / len(pieces), top_value / len(pieces)))
        loudness = loudness * jnp.repeat(draws, shape[position] // shards_of).reshape([-1 if axis == position else 1 for axis in range(len(shape))])
    return loudness


def scatter_about(own_key, dims, scale, limit, split=(), kind=jnp.bfloat16):
    loudness = block_scale(own_key, dims, split, -0.22, 0.18) if split else 1.0
    entries = jax.random.normal(own_key, dims, jnp.float32) * scale * loudness
    return jnp.minimum(jnp.maximum(entries, -limit), limit).astype(kind)


def setup_inputs(seed: int = 0) -> dict:
    arg_keys = jax.random.split(jax.random.key(seed), 8)
    return {
        "hidden": draw_hidden(jax.random.fold_in(arg_keys[7], 71), 0),
        "norm_gain": jnp.clip(1.0 + 0.18 * jax.random.normal(arg_keys[1], (D,), jnp.float32), 0.1, 1.9),
        "query_weight": scatter_about(arg_keys[2], (D, HEADS * HEAD_DIM), D ** -0.5, 0.125, ((1, 2),)),
        "key_weight": scatter_about(arg_keys[3], (D, KV_HEADS * HEAD_DIM), D ** -0.5, 0.125),
        "value_weight": scatter_about(arg_keys[4], (D, KV_HEADS * HEAD_DIM), D ** -0.5, 0.125),
        "head_bias": draw_head_bias(jax.random.fold_in(arg_keys[7], 71), 0),
        "output_weight": scatter_about(arg_keys[6], (HEADS * HEAD_DIM, D), (HEADS * HEAD_DIM) ** -0.5, 0.1875, ((0, 2),)),
    }


def reference(hidden, norm_gain, query_weight, key_weight, value_weight, head_bias, output_weight):
    group = HEADS // KV_HEADS
    scale = HEAD_DIM ** (-0.5)
    wide = hidden.astype(jnp.float32)
    normed = (wide * lax.rsqrt(lax.optimization_barrier(jnp.mean(wide * wide, axis=-1, keepdims=True)) + 1e-06) * norm_gain).astype(jnp.bfloat16)
    queries = jnp.dot(normed, query_weight, preferred_element_type=jnp.float32).astype(jnp.bfloat16)
    keys = jnp.dot(normed, key_weight, preferred_element_type=jnp.float32).astype(jnp.bfloat16)
    values = jnp.dot(normed, value_weight, preferred_element_type=jnp.float32).astype(jnp.bfloat16)
    key_heads = jnp.repeat(keys.reshape(TOKENS, KV_HEADS, HEAD_DIM), group, axis=1).astype(jnp.float32)
    value_heads = jnp.repeat(values.reshape(TOKENS, KV_HEADS, HEAD_DIM), group, axis=1).astype(jnp.float32)
    qblock = math.gcd(TOKENS, 256)
    blocks = TOKENS // qblock
    query_blocks = queries.reshape(blocks, qblock, HEADS, HEAD_DIM)
    query_pos = jnp.arange(TOKENS, dtype=jnp.int32).reshape(blocks, qblock)
    key_pos = jnp.arange(TOKENS, dtype=jnp.int32)

    def one_block(args):
        qblk, qpos = args
        z = jnp.einsum('qhd,khd->hqk', qblk.astype(jnp.float32), key_heads) * scale
        z = z + head_bias[:, None, None]
        strict = (key_pos[None, :] < qpos[:, None])[None, :, :]
        keep = jnp.where(strict, jax.nn.log_sigmoid(-z), 0.0)
        between = lax.cumsum(keep, axis=2, reverse=True) - keep
        weight = jnp.where(strict, jnp.exp(jax.nn.log_sigmoid(z) + between), 0.0).astype(jnp.bfloat16)
        out = jnp.einsum('hqk,khd->qhd', weight.astype(jnp.float32), value_heads)
        return out.astype(jnp.bfloat16)
    attended = lax.map(one_block, (query_blocks, query_pos)).reshape(TOKENS, HEADS * HEAD_DIM)
    return jnp.dot(attended, output_weight, preferred_element_type=jnp.float32).astype(jnp.bfloat16)
```

```python
import functools
import math

import jax
import jax.numpy as jnp
from jax import lax
from jax.experimental import pallas as pl
from jax.experimental.pallas import tpu as pltpu
from jax.sharding import PartitionSpec as P

HEADS = 16
KV_HEADS = 4
HEAD_DIM = 64
LOG2E = math.log2(math.e)


def attend_kernel(span, kv_count, share, bias_ref, q_ref, pairs_ref, out_ref, heads_q, total, kept, tri):
    rows = q_ref.shape[0]
    heads = kv_count * share
    kv_width = kv_count * HEAD_DIM
    offset = lax.axis_index("sp") * rows
    for h in range(heads):
        heads_q[h] = q_ref[:, h * HEAD_DIM : (h + 1) * HEAD_DIM]
    total[...] = jnp.zeros_like(total)
    kept[...] = jnp.zeros_like(kept)
    above = lax.broadcasted_iota(jnp.int32, (span, span), 0)
    below = lax.broadcasted_iota(jnp.int32, (span, span), 1)
    tri[...] = (above > below).astype(jnp.float32).astype(jnp.bfloat16)

    def chunk(start, masked):
        start = pl.multiple_of(start, span)
        block = pairs_ref[pl.ds(start, span), :]
        if masked:
            key_pos = start + lax.broadcasted_iota(jnp.int32, (rows, span), 1)
            query_pos = offset + lax.broadcasted_iota(jnp.int32, (rows, span), 0)
            strict = key_pos < query_pos
        later = tri[...]
        for g in range(kv_count):
            key_block = block[:, g * HEAD_DIM : (g + 1) * HEAD_DIM]
            value_block = block[:, kv_width + g * HEAD_DIM : kv_width + (g + 1) * HEAD_DIM]
            for r in range(share):
                h = g * share + r
                dots = lax.dot_general(
                    heads_q[h], key_block, (((1,), (1,)), ((), ())), preferred_element_type=jnp.float32
                )
                u = dots * (HEAD_DIM ** (-0.5) * LOG2E) + bias_ref[h] * LOG2E
                drop = jnp.maximum(u, jnp.log2(1.0 + jnp.exp2(jnp.minimum(u, 126.0))))
                if masked:
                    drop = jnp.where(strict, drop, 0.0)
                after = jnp.dot(drop.astype(jnp.bfloat16), later, preferred_element_type=jnp.float32)
                before = kept[h][:, :1]
                power = (u - drop) - (after + before)
                weight = jnp.exp2(power)
                if masked:
                    weight = jnp.where(strict, weight, 0.0)
                total[h] += jnp.dot(
                    weight.astype(jnp.bfloat16), value_block, preferred_element_type=jnp.float32
                )
                kept[h] = jnp.broadcast_to(before + (after[:, :1] + drop[:, :1]), kept.shape[1:])

    whole = offset // span
    turns = (offset + rows + span - 1) // span

    def edge(turn, _):
        chunk((turns - 1 - turn) * span, True)
        return 0

    def plain(turn, _):
        chunk((whole - 1 - turn) * span, False)
        return 0

    lax.fori_loop(0, turns - whole, edge, 0)
    lax.fori_loop(0, whole, plain, 0)
    for h in range(heads):
        out_ref[:, h * HEAD_DIM : (h + 1) * HEAD_DIM] = total[h].astype(jnp.bfloat16)


def local(hidden, norm_gain, query_weight, key_weight, value_weight, head_bias, output_weight):
    group = HEADS // KV_HEADS
    local_heads = query_weight.shape[1] // HEAD_DIM
    kv_count = max(1, local_heads // group)
    share = min(local_heads, group)
    first = lax.axis_index("tp") * local_heads // group
    key_cols = lax.dynamic_slice_in_dim(key_weight, first * HEAD_DIM, kv_count * HEAD_DIM, 1)
    value_cols = lax.dynamic_slice_in_dim(value_weight, first * HEAD_DIM, kv_count * HEAD_DIM, 1)
    wide = hidden.astype(jnp.float32)
    normed = (
        wide * lax.rsqrt(jnp.mean(wide * wide, axis=-1, keepdims=True) + 1e-06) * norm_gain
    ).astype(jnp.bfloat16)
    joined = jnp.concatenate([key_cols, value_cols], axis=1)
    key_value = jnp.dot(normed, joined, preferred_element_type=jnp.float32).astype(jnp.bfloat16)
    all_pairs = lax.all_gather(key_value, "sp", axis=0, tiled=True)
    queries = jnp.dot(normed, query_weight, preferred_element_type=jnp.float32).astype(jnp.bfloat16)
    rows = queries.shape[0]
    span = math.gcd(all_pairs.shape[0], 256)
    heads = local_heads
    attended = pl.pallas_call(
        functools.partial(attend_kernel, span, kv_count, share),
        out_shape=jax.ShapeDtypeStruct((rows, heads * HEAD_DIM), jnp.bfloat16),
        in_specs=[
            pl.BlockSpec(memory_space=pltpu.SMEM),
            pl.BlockSpec(memory_space=pltpu.VMEM),
            pl.BlockSpec(memory_space=pltpu.VMEM),
        ],
        out_specs=pl.BlockSpec(memory_space=pltpu.VMEM),
        scratch_shapes=[
            pltpu.VMEM((heads, rows, HEAD_DIM), jnp.bfloat16),
            pltpu.VMEM((heads, rows, HEAD_DIM), jnp.float32),
            pltpu.VMEM((heads, rows, 128), jnp.float32),
            pltpu.VMEM((span, span), jnp.bfloat16),
        ],
        cost_estimate=pl.CostEstimate(flops=2000000000, bytes_accessed=4000000, transcendentals=10000000),
    )(head_bias, queries, all_pairs)
    every_head = lax.all_gather(attended, "tp", axis=1, tiled=True)
    summed = jnp.dot(
        every_head,
        lax.all_gather(output_weight, "tp", axis=0, tiled=True),
        preferred_element_type=jnp.float32,
    )
    return summed.astype(jnp.bfloat16)


def solution(mesh):
    placed = (P("sp", None), P(), P(None, "tp"), P(), P(), P("tp"), P("tp", None))
    return jax.shard_map(
        local, mesh=mesh, in_specs=placed, out_specs=P("sp", None), check_vma=False
    )
```

```python
import functools
import math

import jax
import jax.numpy as jnp
from jax import lax
from jax.experimental import pallas as pl
from jax.experimental.pallas import tpu as pltpu
from jax.sharding import PartitionSpec as P

HEADS = 16
KV_HEADS = 4
HEAD_DIM = 64
LOG2E = math.log2(math.e)


PLANE = 4
MESH = pl.DeviceIdType.MESH


def layer_kernel(
    span, kv_count, share, devices, ranks,
    bias_ref, q_ref, kv_ref, mix_ref, out_ref,
    pairs, spare, heads_q, total, kept, tri, gathered, mixers,
    arrive, spare_arrive, up_sem, side_sem, over_sem, own_sem, mix_send, mix_arrive, mix_local, att_send, att_arrive,
):
    rows = q_ref.shape[0]
    heads = kv_count * share
    kv_width = kv_count * HEAD_DIM
    me = lax.axis_index("sp")
    rank = lax.axis_index("tp")
    levels = devices // PLANE
    level = me // PLANE
    place = me % PLANE
    across = PLANE - 1 - place
    side = place + 1 - 2 * (place % 2)
    over = (place + 2) % PLANE
    has_up = level < levels - 1
    offset = me * rows

    def slot(block):
        return pairs.at[pl.ds(pl.multiple_of(block * rows, 16), rows), :]

    def ship(source, block, send, target):
        return pltpu.make_async_remote_copy(
            src_ref=source, dst_ref=slot(block), send_sem=send, recv_sem=arrive.at[block],
            device_id={"sp": target}, device_id_type=MESH,
        )

    def own_to(index, where):
        return ship(kv_ref, me, own_sem.at[index], level * PLANE + where)

    def own_spare():
        return pltpu.make_async_remote_copy(
            src_ref=kv_ref, dst_ref=spare, send_sem=own_sem.at[2], recv_sem=spare_arrive,
            device_id={"sp": level * PLANE + across}, device_id_type=MESH,
        )

    def lift_up():
        return ship(spare, level * PLANE + across, up_sem.at[level * PLANE + across], me + PLANE)

    def own_up():
        return ship(kv_ref, me, up_sem.at[me], me + PLANE)

    def send_up(block):
        return ship(slot(block), block, up_sem.at[block], me + PLANE)

    def send_side(block):
        return ship(slot(block), block, side_sem.at[block], level * PLANE + side)

    def send_over(block):
        return ship(slot(block), block, over_sem.at[block], level * PLANE + over)

    def mixer(step):
        return pltpu.make_async_remote_copy(
            src_ref=mix_ref, dst_ref=mixers.at[rank], send_sem=mix_send.at[step],
            recv_sem=mix_arrive.at[step], device_id={"tp": (rank + step) % ranks}, device_id_type=MESH,
        )

    def attended(step):
        return pltpu.make_async_remote_copy(
            src_ref=gathered.at[rank], dst_ref=gathered.at[rank], send_sem=att_send.at[step],
            recv_sem=att_arrive.at[step], device_id={"tp": (rank + step) % ranks}, device_id_type=MESH,
        )

    pl.when(side > place)(lambda: own_to(0, side).start())
    pl.when(over > place)(lambda: own_to(1, over).start())
    pl.when(has_up)(lambda: own_up().start())
    pl.when(across > place)(lambda: own_to(2, across).start())
    pl.when((across < place) & has_up)(lambda: own_spare().start())
    mine = pltpu.make_async_copy(mix_ref, mixers.at[rank], mix_local)
    mine.start()
    for step in range(1, ranks):
        mixer(step).start()

    pairs[pl.ds(pl.multiple_of(offset, 16), rows), :] = kv_ref[...]
    for h in range(heads):
        heads_q[h] = q_ref[:, h * HEAD_DIM : (h + 1) * HEAD_DIM]
    total[...] = jnp.zeros_like(total)
    kept[...] = jnp.zeros_like(kept)
    first_pos = lax.broadcasted_iota(jnp.int32, (span, span), 0)
    second_pos = lax.broadcasted_iota(jnp.int32, (span, span), 1)
    tri[...] = (first_pos > second_pos).astype(jnp.float32).astype(jnp.bfloat16)

    def take(block):
        ship(slot(block), block, up_sem.at[block], (me + 1) % devices).wait_recv()
        spot = block % PLANE
        lower = block // PLANE < level

        def relay_up():
            send_up(block).start()

        def relay_plane():
            send_side(block).start()
            send_over(block).start()

        pl.when(has_up & ((spot == place) | (spot == across)))(relay_up)
        pl.when(lower & (spot == place))(relay_plane)

    def take_until(front, low):
        low = jnp.maximum(low, 0)
        count = jnp.maximum(front - low, 0)

        def one(index, _):
            take(front - 1 - index)
            return 0

        lax.fori_loop(0, count, one, 0)
        return front - count

    def chunk(start, masked):
        start = pl.multiple_of(start, span)
        block = pairs[pl.ds(start, span), :]
        if masked:
            key_pos = start + lax.broadcasted_iota(jnp.int32, (rows, span), 1)
            query_pos = offset + lax.broadcasted_iota(jnp.int32, (rows, span), 0)
            strict = key_pos < query_pos
            value_pos = start + lax.broadcasted_iota(jnp.int32, (span, block.shape[1]), 0)
            block = jnp.where(value_pos < offset + rows, block.astype(jnp.float32), 0.0)
            block = block.astype(jnp.bfloat16)
        later = tri[...]
        for g in range(kv_count):
            key_block = block[:, g * HEAD_DIM : (g + 1) * HEAD_DIM]
            value_block = block[:, kv_width + g * HEAD_DIM : kv_width + (g + 1) * HEAD_DIM]
            for r in range(share):
                h = g * share + r
                dots = lax.dot_general(
                    heads_q[h], key_block, (((1,), (1,)), ((), ())), preferred_element_type=jnp.float32
                )
                u = dots * (HEAD_DIM ** (-0.5) * LOG2E) + bias_ref[h] * LOG2E
                drop = jnp.maximum(u, jnp.log2(1.0 + jnp.exp2(jnp.minimum(u, 126.0))))
                if masked:
                    drop = jnp.where(strict, drop, 0.0)
                after = jnp.dot(drop.astype(jnp.bfloat16), later, preferred_element_type=jnp.float32)
                before = kept[h][:, :1]
                weight = jnp.exp2((u - drop) - (after + before))
                if masked:
                    weight = jnp.where(strict, weight, 0.0)
                total[h] += jnp.dot(
                    weight.astype(jnp.bfloat16), value_block, preferred_element_type=jnp.float32
                )
                kept[h] = jnp.broadcast_to(before + (after[:, :1] + drop[:, :1]), kept.shape[1:])

    whole = offset // span
    turns = (offset + rows + span - 1) // span

    def edge(turn, front):
        start = (turns - 1 - turn) * span
        front = take_until(front, start // rows)
        chunk(start, True)
        return front

    def plain(turn, front):
        start = (whole - 1 - turn) * span
        front = take_until(front, (start - span) // rows)
        chunk(start, False)
        return front

    front = lax.fori_loop(0, turns - whole, edge, me)

    def lift():
        own_spare().wait_recv()
        lift_up().start()

    pl.when(has_up & (across > place))(lift)
    front = lax.fori_loop(0, whole, plain, front)
    take_until(front, 0)

    for h in range(heads):
        gathered[rank, :, h * HEAD_DIM : (h + 1) * HEAD_DIM] = total[h].astype(jnp.bfloat16)
    for step in range(1, ranks):
        attended(step).start()
    mine.wait()
    for step in range(1, ranks):
        mixer(step).wait_recv()
    for step in range(1, ranks):
        attended(step).wait_recv()
    features = out_ref.shape[1]
    tile = math.gcd(features, 512)
    for column in range(0, features, tile):
        summed = jnp.zeros((rows, tile), jnp.float32)
        for r in range(ranks):
            summed += jnp.dot(
                gathered[r], mixers[r, :, column : column + tile], preferred_element_type=jnp.float32
            )
        out_ref[:, column : column + tile] = summed.astype(jnp.bfloat16)

    pl.when(side > place)(lambda: own_to(0, side).wait_send())
    pl.when(over > place)(lambda: own_to(1, over).wait_send())
    pl.when(across > place)(lambda: own_to(2, across).wait_send())
    pl.when((across < place) & has_up)(lambda: own_spare().wait_send())
    pl.when(has_up)(lambda: own_up().wait_send())
    pl.when(has_up & (across > place))(lambda: lift_up().wait_send())

    def settle(block, _):
        spot = block % PLANE
        lower = block // PLANE < level

        def plane_done():
            send_side(block).wait_send()
            send_over(block).wait_send()

        pl.when(has_up & ((spot == place) | (spot == across)))(lambda: send_up(block).wait_send())
        pl.when(lower & (spot == place))(plane_done)
        return 0

    lax.fori_loop(0, me, settle, 0)
    for step in range(1, ranks):
        mixer(step).wait_send()
        attended(step).wait_send()


def local(hidden, norm_gain, query_weight, key_weight, value_weight, head_bias, output_weight):
    group = HEADS // KV_HEADS
    local_heads = query_weight.shape[1] // HEAD_DIM
    kv_count = max(1, local_heads // group)
    share = min(local_heads, group)
    first = lax.axis_index("tp") * local_heads // group
    key_cols = lax.dynamic_slice_in_dim(key_weight, first * HEAD_DIM, kv_count * HEAD_DIM, 1)
    value_cols = lax.dynamic_slice_in_dim(value_weight, first * HEAD_DIM, kv_count * HEAD_DIM, 1)
    wide = hidden.astype(jnp.float32)
    normed = (
        wide * lax.rsqrt(jnp.mean(wide * wide, axis=-1, keepdims=True) + 1e-06) * norm_gain
    ).astype(jnp.bfloat16)
    joined = jnp.concatenate([key_cols, value_cols], axis=1)
    key_value = jnp.dot(normed, joined, preferred_element_type=jnp.float32).astype(jnp.bfloat16)
    queries = jnp.dot(normed, query_weight, preferred_element_type=jnp.float32).astype(jnp.bfloat16)
    rows = queries.shape[0]
    devices = lax.axis_size("sp")
    ranks = lax.axis_size("tp")
    span = math.gcd(rows * devices, 256)
    width = query_weight.shape[1]
    features = output_weight.shape[1]
    vmem = pl.BlockSpec(memory_space=pltpu.VMEM)
    dma = pltpu.SemaphoreType.DMA
    return pl.pallas_call(
        functools.partial(layer_kernel, span, kv_count, share, devices, ranks),
        out_shape=jax.ShapeDtypeStruct((rows, features), jnp.bfloat16),
        in_specs=[
            pl.BlockSpec(memory_space=pltpu.SMEM),
            vmem,
            vmem,
            pl.BlockSpec(memory_space=pl.ANY),
        ],
        out_specs=vmem,
        scratch_shapes=[
            pltpu.VMEM((rows * devices, key_value.shape[1]), jnp.bfloat16),
            pltpu.VMEM(key_value.shape, jnp.bfloat16),
            pltpu.VMEM((local_heads, rows, HEAD_DIM), jnp.bfloat16),
            pltpu.VMEM((local_heads, rows, HEAD_DIM), jnp.float32),
            pltpu.VMEM((local_heads, rows, 128), jnp.float32),
            pltpu.VMEM((span, span), jnp.bfloat16),
            pltpu.VMEM((ranks, rows, width), jnp.bfloat16),
            pltpu.VMEM((ranks, width, features), jnp.bfloat16),
            dma((devices,)),
            dma,
            dma((devices,)),
            dma((devices,)),
            dma((devices,)),
            dma((3,)),
            dma((ranks,)),
            dma((ranks,)),
            dma,
            dma((ranks,)),
            dma((ranks,)),
        ],
        compiler_params=pltpu.CompilerParams(has_side_effects=True),
    )(head_bias, queries, key_value, output_weight)


def solution(mesh):
    placed = (P("sp", None), P(), P(None, "tp"), P(), P(), P("tp"), P("tp", None))
    return jax.shard_map(
        local, mesh=mesh, in_specs=placed, out_specs=P("sp", None), check_vma=False
    )
```

```python
import functools
import math

import jax
import jax.numpy as jnp
from jax import lax
from jax.experimental import pallas as pl
from jax.experimental.pallas import tpu as pltpu
from jax.sharding import PartitionSpec as P

HEADS = 16
KV_HEADS = 4
HEAD_DIM = 64
LOG2E = math.log2(math.e)


PLANE = 4
PACE = 2
MESH = pl.DeviceIdType.MESH


def layer_kernel(
    span, kv_count, share, devices, ranks,
    bias_ref, q_ref, kv_ref, mix_ref, out_ref,
    pairs, spare, heads_q, total, kept, tri, gathered, mixers,
    arrive, spare_arrive, up_sem, side_sem, over_sem, own_sem, mix_send, mix_arrive, mix_local, att_send, att_arrive,
):
    rows = q_ref.shape[0]
    heads = kv_count * share
    kv_width = kv_count * HEAD_DIM
    me = lax.axis_index("sp")
    rank = lax.axis_index("tp")
    levels = devices // PLANE
    level = me // PLANE
    place = me % PLANE
    across = PLANE - 1 - place
    side = place + 1 - 2 * (place % 2)
    over = (place + 2) % PLANE
    has_up = level < levels - 1
    offset = me * rows

    def slot(block):
        return pairs.at[pl.ds(pl.multiple_of(block * rows, 16), rows), :]

    def ship(source, block, send, target):
        return pltpu.make_async_remote_copy(
            src_ref=source, dst_ref=slot(block), send_sem=send, recv_sem=arrive.at[block],
            device_id={"sp": target}, device_id_type=MESH,
        )

    def own_to(index, where):
        return ship(kv_ref, me, own_sem.at[index], level * PLANE + where)

    def own_spare():
        return pltpu.make_async_remote_copy(
            src_ref=kv_ref, dst_ref=spare, send_sem=own_sem.at[2], recv_sem=spare_arrive,
            device_id={"sp": level * PLANE + across}, device_id_type=MESH,
        )

    def lift_up():
        return ship(spare, level * PLANE + across, up_sem.at[level * PLANE + across], me + PLANE)

    def own_up():
        return ship(kv_ref, me, up_sem.at[me], me + PLANE)

    def send_up(block):
        return ship(slot(block), block, up_sem.at[block], me + PLANE)

    def send_side(block):
        return ship(slot(block), block, side_sem.at[block], level * PLANE + side)

    def send_over(block):
        return ship(slot(block), block, over_sem.at[block], level * PLANE + over)

    def mixer(step):
        return pltpu.make_async_remote_copy(
            src_ref=mix_ref, dst_ref=mixers.at[rank], send_sem=mix_send.at[step],
            recv_sem=mix_arrive.at[step], device_id={"tp": (rank + step) % ranks}, device_id_type=MESH,
        )

    def attended(step):
        return pltpu.make_async_remote_copy(
            src_ref=gathered.at[rank], dst_ref=gathered.at[rank], send_sem=att_send.at[step],
            recv_sem=att_arrive.at[step], device_id={"tp": (rank + step) % ranks}, device_id_type=MESH,
        )

    pl.when(side > place)(lambda: own_to(0, side).start())
    pl.when(over > place)(lambda: own_to(1, over).start())
    pl.when(has_up)(lambda: own_up().start())
    pl.when(across > place)(lambda: own_to(2, across).start())
    pl.when((across < place) & has_up)(lambda: own_spare().start())
    mine = pltpu.make_async_copy(mix_ref, mixers.at[rank], mix_local)
    mine.start()
    for step in range(1, ranks):
        mixer(step).start()

    pairs[pl.ds(pl.multiple_of(offset, 16), rows), :] = kv_ref[...]
    for h in range(heads):
        heads_q[h] = q_ref[:, h * HEAD_DIM : (h + 1) * HEAD_DIM]
    total[...] = jnp.zeros_like(total)
    kept[...] = jnp.zeros_like(kept)
    first_pos = lax.broadcasted_iota(jnp.int32, (span, span), 0)
    second_pos = lax.broadcasted_iota(jnp.int32, (span, span), 1)
    tri[...] = (first_pos > second_pos).astype(jnp.float32).astype(jnp.bfloat16)

    def arrived(block):
        ship(slot(block), block, up_sem.at[block], (me + 1) % devices).wait_recv()

    def relay_column(block):
        arrived(block)
        pl.when(has_up)(lambda: send_up(block).start())
        send_side(block).start()
        send_over(block).start()

    def relay_across(block):
        arrived(block)
        pl.when(has_up)(lambda: send_up(block).start())

    def lift():
        own_spare().wait_recv()
        lift_up().start()

    def relay(group):
        pl.when((group == 0) & has_up & (across > place))(lift)
        lower = level - group
        held = lower * PLANE + across
        pl.when((group > 0) | (across < place))(lambda: relay_across(held))
        pl.when(lower >= 1)(lambda: relay_column((lower - 1) * PLANE + place))

    def relay_until(done, count):
        count = jnp.minimum(count, level + 1)
        ahead = jnp.maximum(count - done, 0)

        def one(index, _):
            relay(done + index)
            return 0

        lax.fori_loop(0, ahead, one, 0)
        return done + ahead

    def take_until(front, low):
        count = jnp.maximum(front - low, 0)

        def one(index, _):
            block = front - 1 - index
            spot = block % PLANE
            pl.when((spot != place) & (spot != across))(lambda: arrived(block))
            return 0

        lax.fori_loop(0, count, one, 0)
        return front - count

    def advance(state, start, turn):
        done, front = state
        low = start // rows
        done = relay_until(done, jnp.maximum(turn // PACE + 1, level - low // PLANE + 1))
        return done, take_until(front, low)

    def chunk(start, masked):
        start = pl.multiple_of(start, span)
        block = pairs[pl.ds(start, span), :]
        if masked:
            key_pos = start + lax.broadcasted_iota(jnp.int32, (rows, span), 1)
            query_pos = offset + lax.broadcasted_iota(jnp.int32, (rows, span), 0)
            strict = key_pos < query_pos
            value_pos = start + lax.broadcasted_iota(jnp.int32, (span, block.shape[1]), 0)
            block = jnp.where(value_pos < offset + rows, block.astype(jnp.float32), 0.0)
            block = block.astype(jnp.bfloat16)
        later = tri[...]
        for g in range(kv_count):
            key_block = block[:, g * HEAD_DIM : (g + 1) * HEAD_DIM]
            value_block = block[:, kv_width + g * HEAD_DIM : kv_width + (g + 1) * HEAD_DIM]
            for r in range(share):
                h = g * share + r
                dots = lax.dot_general(
                    heads_q[h], key_block, (((1,), (1,)), ((), ())), preferred_element_type=jnp.float32
                )
                u = dots * (HEAD_DIM ** (-0.5) * LOG2E) + bias_ref[h] * LOG2E
                drop = jnp.maximum(u, jnp.log2(1.0 + jnp.exp2(jnp.minimum(u, 126.0))))
                if masked:
                    drop = jnp.where(strict, drop, 0.0)
                after = jnp.dot(drop.astype(jnp.bfloat16), later, preferred_element_type=jnp.float32)
                before = kept[h][:, :1]
                weight = jnp.exp2((u - drop) - (after + before))
                if masked:
                    weight = jnp.where(strict, weight, 0.0)
                total[h] += jnp.dot(
                    weight.astype(jnp.bfloat16), value_block, preferred_element_type=jnp.float32
                )
                kept[h] = jnp.broadcast_to(before + (after[:, :1] + drop[:, :1]), kept.shape[1:])

    whole = offset // span
    turns = (offset + rows + span - 1) // span

    def edge(turn, state):
        start = (turns - 1 - turn) * span
        state = advance(state, start, turn)
        chunk(start, True)
        return state

    def plain(turn, state):
        start = (whole - 1 - turn) * span
        state = advance(state, start, turn + turns - whole)
        chunk(start, False)
        return state

    state = lax.fori_loop(0, turns - whole, edge, (0, me))
    done, front = lax.fori_loop(0, whole, plain, state)
    relay_until(done, level + 1)
    take_until(front, 0)

    for h in range(heads):
        gathered[rank, :, h * HEAD_DIM : (h + 1) * HEAD_DIM] = total[h].astype(jnp.bfloat16)
    for step in range(1, ranks):
        attended(step).start()
    mine.wait()
    for step in range(1, ranks):
        mixer(step).wait_recv()
    for step in range(1, ranks):
        attended(step).wait_recv()
    features = out_ref.shape[1]
    tile = math.gcd(features, 512)
    for column in range(0, features, tile):
        summed = jnp.zeros((rows, tile), jnp.float32)
        for r in range(ranks):
            summed += jnp.dot(
                gathered[r], mixers[r, :, column : column + tile], preferred_element_type=jnp.float32
            )
        out_ref[:, column : column + tile] = summed.astype(jnp.bfloat16)

    pl.when(side > place)(lambda: own_to(0, side).wait_send())
    pl.when(over > place)(lambda: own_to(1, over).wait_send())
    pl.when(across > place)(lambda: own_to(2, across).wait_send())
    pl.when((across < place) & has_up)(lambda: own_spare().wait_send())
    pl.when(has_up)(lambda: own_up().wait_send())
    pl.when(has_up & (across > place))(lambda: lift_up().wait_send())

    def settle(block, _):
        spot = block % PLANE
        lower = block // PLANE < level

        def plane_done():
            send_side(block).wait_send()
            send_over(block).wait_send()

        pl.when(has_up & ((spot == place) | (spot == across)))(lambda: send_up(block).wait_send())
        pl.when(lower & (spot == place))(plane_done)
        return 0

    lax.fori_loop(0, me, settle, 0)
    for step in range(1, ranks):
        mixer(step).wait_send()
        attended(step).wait_send()


def local(hidden, norm_gain, query_weight, key_weight, value_weight, head_bias, output_weight):
    group = HEADS // KV_HEADS
    local_heads = query_weight.shape[1] // HEAD_DIM
    kv_count = max(1, local_heads // group)
    share = min(local_heads, group)
    first = lax.axis_index("tp") * local_heads // group
    key_cols = lax.dynamic_slice_in_dim(key_weight, first * HEAD_DIM, kv_count * HEAD_DIM, 1)
    value_cols = lax.dynamic_slice_in_dim(value_weight, first * HEAD_DIM, kv_count * HEAD_DIM, 1)
    wide = hidden.astype(jnp.float32)
    normed = (
        wide * lax.rsqrt(jnp.mean(wide * wide, axis=-1, keepdims=True) + 1e-06) * norm_gain
    ).astype(jnp.bfloat16)
    joined = jnp.concatenate([key_cols, value_cols], axis=1)
    key_value = jnp.dot(normed, joined, preferred_element_type=jnp.float32).astype(jnp.bfloat16)
    queries = jnp.dot(normed, query_weight, preferred_element_type=jnp.float32).astype(jnp.bfloat16)
    rows = queries.shape[0]
    devices = lax.axis_size("sp")
    ranks = lax.axis_size("tp")
    span = math.gcd(rows * devices, 256)
    width = query_weight.shape[1]
    features = output_weight.shape[1]
    vmem = pl.BlockSpec(memory_space=pltpu.VMEM)
    dma = pltpu.SemaphoreType.DMA
    return pl.pallas_call(
        functools.partial(layer_kernel, span, kv_count, share, devices, ranks),
        out_shape=jax.ShapeDtypeStruct((rows, features), jnp.bfloat16),
        in_specs=[
            pl.BlockSpec(memory_space=pltpu.SMEM),
            vmem,
            vmem,
            pl.BlockSpec(memory_space=pl.ANY),
        ],
        out_specs=vmem,
        scratch_shapes=[
            pltpu.VMEM((rows * devices, key_value.shape[1]), jnp.bfloat16),
            pltpu.VMEM(key_value.shape, jnp.bfloat16),
            pltpu.VMEM((local_heads, rows, HEAD_DIM), jnp.bfloat16),
            pltpu.VMEM((local_heads, rows, HEAD_DIM), jnp.float32),
            pltpu.VMEM((local_heads, rows, 128), jnp.float32),
            pltpu.VMEM((span, span), jnp.bfloat16),
            pltpu.VMEM((ranks, rows, width), jnp.bfloat16),
            pltpu.VMEM((ranks, width, features), jnp.bfloat16),
            dma((devices,)),
            dma,
            dma((devices,)),
            dma((devices,)),
            dma((devices,)),
            dma((3,)),
            dma((ranks,)),
            dma((ranks,)),
            dma,
            dma((ranks,)),
            dma((ranks,)),
        ],
        compiler_params=pltpu.CompilerParams(has_side_effects=True),
    )(head_bias, queries, key_value, output_weight)


def solution(mesh):
    placed = (P("sp", None), P(), P(None, "tp"), P(), P(), P("tp"), P("tp", None))
    return jax.shard_map(
        local, mesh=mesh, in_specs=placed, out_specs=P("sp", None), check_vma=False
    )
```

```python
import functools
import math

import jax
import jax.numpy as jnp
from jax import lax
from jax.experimental import pallas as pl
from jax.experimental.pallas import tpu as pltpu
from jax.sharding import PartitionSpec as P

HEADS = 16
KV_HEADS = 4
HEAD_DIM = 64
LOG2E = math.log2(math.e)


PLANE = 4
PACE = 2
ROWS = 192
LAG = 8
MESH = pl.DeviceIdType.MESH


def layer_kernel(
    span, kv_count, share, devices, ranks,
    bias_ref, q_ref, kv_ref, mix_ref, out_ref,
    pairs, spare, heads_q, total, kept, gain, lost, tri, gathered, mixers,
    arrive, spare_arrive, up_sem, side_sem, over_sem, own_sem, mix_send, mix_arrive, mix_local, att_send, att_arrive,
):
    rows = q_ref.shape[0]
    heads = kv_count * share
    kv_width = kv_count * HEAD_DIM
    me = lax.axis_index("sp")
    rank = lax.axis_index("tp")
    levels = devices // PLANE
    level = me // PLANE
    place = me % PLANE
    across = PLANE - 1 - place
    side = place + 1 - 2 * (place % 2)
    over = (place + 2) % PLANE
    has_up = level < levels - 1
    offset = me * rows

    def slot(block):
        return pairs.at[pl.ds(pl.multiple_of(block * rows, 16), rows), :]

    def ship(source, block, send, target):
        return pltpu.make_async_remote_copy(
            src_ref=source, dst_ref=slot(block), send_sem=send, recv_sem=arrive.at[block],
            device_id={"sp": target}, device_id_type=MESH,
        )

    def own_to(index, where):
        return ship(kv_ref, me, own_sem.at[index], level * PLANE + where)

    def own_spare():
        return pltpu.make_async_remote_copy(
            src_ref=kv_ref, dst_ref=spare, send_sem=own_sem.at[2], recv_sem=spare_arrive,
            device_id={"sp": level * PLANE + across}, device_id_type=MESH,
        )

    def lift_up():
        return ship(spare, level * PLANE + across, up_sem.at[level * PLANE + across], me + PLANE)

    def own_up():
        return ship(kv_ref, me, up_sem.at[me], me + PLANE)

    def send_up(block):
        return ship(slot(block), block, up_sem.at[block], me + PLANE)

    def send_side(block):
        return ship(slot(block), block, side_sem.at[block], level * PLANE + side)

    def send_over(block):
        return ship(slot(block), block, over_sem.at[block], level * PLANE + over)

    def mixer(step):
        return pltpu.make_async_remote_copy(
            src_ref=mix_ref, dst_ref=mixers.at[rank], send_sem=mix_send.at[step],
            recv_sem=mix_arrive.at[step], device_id={"tp": (rank + step) % ranks}, device_id_type=MESH,
        )

    def attended(step):
        return pltpu.make_async_remote_copy(
            src_ref=gathered.at[rank], dst_ref=gathered.at[rank], send_sem=att_send.at[step],
            recv_sem=att_arrive.at[step], device_id={"tp": (rank + step) % ranks}, device_id_type=MESH,
        )

    pl.when(side > place)(lambda: own_to(0, side).start())
    pl.when(over > place)(lambda: own_to(1, over).start())
    pl.when(has_up)(lambda: own_up().start())
    pl.when(across > place)(lambda: own_to(2, across).start())
    pl.when((across < place) & has_up)(lambda: own_spare().start())
    mine = pltpu.make_async_copy(mix_ref, mixers.at[rank], mix_local)
    mine.start()
    for step in range(1, ranks):
        mixer(step).start()

    pairs[pl.ds(pl.multiple_of(offset, 16), rows), :] = kv_ref[...]
    for h in range(heads):
        heads_q[h] = q_ref[:, h * HEAD_DIM : (h + 1) * HEAD_DIM]
    total[...] = jnp.zeros_like(total)
    kept[...] = jnp.zeros_like(kept)
    first_pos = lax.broadcasted_iota(jnp.int32, (span, span), 0)
    second_pos = lax.broadcasted_iota(jnp.int32, (span, span), 1)
    tri[...] = (first_pos > second_pos).astype(jnp.float32).astype(jnp.bfloat16)

    def arrived(block):
        ship(slot(block), block, up_sem.at[block], (me + 1) % devices).wait_recv()

    def relay_column(block):
        arrived(block)
        pl.when(has_up)(lambda: send_up(block).start())
        send_side(block).start()
        send_over(block).start()

    def relay_across(block):
        arrived(block)
        pl.when(has_up)(lambda: send_up(block).start())

    def lift():
        own_spare().wait_recv()
        lift_up().start()

    def relay(group):
        pl.when((group == 0) & has_up & (across > place))(lift)
        lower = level - group
        held = lower * PLANE + across
        pl.when((group > 0) | (across < place))(lambda: relay_across(held))
        pl.when(lower >= 1)(lambda: relay_column((lower - 1) * PLANE + place))

    def relay_until(done, count):
        count = jnp.minimum(count, level + 1)
        ahead = jnp.maximum(count - done, 0)

        def one(index, _):
            relay(done + index)
            return 0

        lax.fori_loop(0, ahead, one, 0)
        return done + ahead

    def take_until(front, low):
        count = jnp.maximum(front - low, 0)

        def one(index, _):
            block = front - 1 - index
            spot = block % PLANE
            pl.when((spot != place) & (spot != across))(lambda: arrived(block))
            return 0

        lax.fori_loop(0, count, one, 0)
        return front - count

    def advance(state, start, turn):
        done, front = state
        low = start // rows
        done = relay_until(done, jnp.maximum(turn // PACE + 1, level - low // PLANE + 1))
        return done, take_until(front, low)

    def chunk(start, masked):
        start = pl.multiple_of(start, span)
        block = pairs[pl.ds(start, span), :]
        if masked:
            key_pos = start + lax.broadcasted_iota(jnp.int32, (rows, span), 1)
            query_pos = offset + lax.broadcasted_iota(jnp.int32, (rows, span), 0)
            strict = key_pos < query_pos
            value_pos = start + lax.broadcasted_iota(jnp.int32, (span, block.shape[1]), 0)
            block = jnp.where(value_pos < offset + rows, block.astype(jnp.float32), 0.0)
            block = block.astype(jnp.bfloat16)
        later = tri[...]
        scale = HEAD_DIM ** (-0.5) * LOG2E
        tiles = [(h, t) for h in range(heads) for t in range(0, rows, ROWS)]

        def first(h, t):
            g = h // share
            dots = lax.dot_general(
                heads_q[h, t : t + ROWS], block[:, g * HEAD_DIM : (g + 1) * HEAD_DIM],
                (((1,), (1,)), ((), ())), preferred_element_type=jnp.float32,
            )
            u = dots * scale + bias_ref[h] * LOG2E
            drop = jnp.maximum(u, jnp.log2(1.0 + jnp.exp2(jnp.minimum(u, 126.0))))
            if masked:
                drop = jnp.where(strict[t : t + ROWS], drop, 0.0)
            gain[h, t : t + ROWS] = u - drop
            lost[h, t : t + ROWS] = drop.astype(jnp.bfloat16)
            return drop[:, :1]

        def second(h, t, head):
            g = h // share
            part = slice(t, t + ROWS)
            after = jnp.dot(lost[h, part], later, preferred_element_type=jnp.float32)
            weight = jnp.exp2(gain[h, part] - (after + jnp.tile(kept[h, part], (1, span // 128))))
            if masked:
                weight = jnp.where(strict[part], weight, 0.0)
            kept[h, part] += jnp.broadcast_to(after[:, :1] + head, (ROWS, 128))
            total[h, part] += jnp.dot(
                weight.astype(jnp.bfloat16),
                block[:, kv_width + g * HEAD_DIM : kv_width + (g + 1) * HEAD_DIM],
                preferred_element_type=jnp.float32,
            )

        waiting = []
        for h, t in tiles:
            waiting.append((h, t, first(h, t)))
            if len(waiting) > LAG:
                second(*waiting.pop(0))
        for item in waiting:
            second(*item)

    whole = offset // span
    turns = (offset + rows + span - 1) // span

    def edge(turn, state):
        start = (turns - 1 - turn) * span
        state = advance(state, start, turn)
        chunk(start, True)
        return state

    def plain(turn, state):
        start = (whole - 1 - turn) * span
        state = advance(state, start, turn + turns - whole)
        chunk(start, False)
        return state

    state = lax.fori_loop(0, turns - whole, edge, (0, me))
    done, front = lax.fori_loop(0, whole, plain, state)
    relay_until(done, level + 1)
    take_until(front, 0)

    for h in range(heads):
        gathered[rank, :, h * HEAD_DIM : (h + 1) * HEAD_DIM] = total[h].astype(jnp.bfloat16)
    for step in range(1, ranks):
        attended(step).start()
    mine.wait()
    for step in range(1, ranks):
        mixer(step).wait_recv()
    for step in range(1, ranks):
        attended(step).wait_recv()
    features = out_ref.shape[1]
    tile = math.gcd(features, 512)
    for column in range(0, features, tile):
        summed = jnp.zeros((rows, tile), jnp.float32)
        for r in range(ranks):
            summed += jnp.dot(
                gathered[r], mixers[r, :, column : column + tile], preferred_element_type=jnp.float32
            )
        out_ref[:, column : column + tile] = summed.astype(jnp.bfloat16)

    pl.when(side > place)(lambda: own_to(0, side).wait_send())
    pl.when(over > place)(lambda: own_to(1, over).wait_send())
    pl.when(across > place)(lambda: own_to(2, across).wait_send())
    pl.when((across < place) & has_up)(lambda: own_spare().wait_send())
    pl.when(has_up)(lambda: own_up().wait_send())
    pl.when(has_up & (across > place))(lambda: lift_up().wait_send())

    def settle(block, _):
        spot = block % PLANE
        lower = block // PLANE < level

        def plane_done():
            send_side(block).wait_send()
            send_over(block).wait_send()

        pl.when(has_up & ((spot == place) | (spot == across)))(lambda: send_up(block).wait_send())
        pl.when(lower & (spot == place))(plane_done)
        return 0

    lax.fori_loop(0, me, settle, 0)
    for step in range(1, ranks):
        mixer(step).wait_send()
        attended(step).wait_send()


def local(hidden, norm_gain, query_weight, key_weight, value_weight, head_bias, output_weight):
    group = HEADS // KV_HEADS
    local_heads = query_weight.shape[1] // HEAD_DIM
    kv_count = max(1, local_heads // group)
    share = min(local_heads, group)
    first = lax.axis_index("tp") * local_heads // group
    key_cols = lax.dynamic_slice_in_dim(key_weight, first * HEAD_DIM, kv_count * HEAD_DIM, 1)
    value_cols = lax.dynamic_slice_in_dim(value_weight, first * HEAD_DIM, kv_count * HEAD_DIM, 1)
    wide = hidden.astype(jnp.float32)
    normed = (
        wide * lax.rsqrt(jnp.mean(wide * wide, axis=-1, keepdims=True) + 1e-06) * norm_gain
    ).astype(jnp.bfloat16)
    joined = jnp.concatenate([key_cols, value_cols], axis=1)
    key_value = jnp.dot(normed, joined, preferred_element_type=jnp.float32).astype(jnp.bfloat16)
    queries = jnp.dot(normed, query_weight, preferred_element_type=jnp.float32).astype(jnp.bfloat16)
    rows = queries.shape[0]
    devices = lax.axis_size("sp")
    ranks = lax.axis_size("tp")
    span = math.gcd(rows * devices, 256)
    width = query_weight.shape[1]
    features = output_weight.shape[1]
    vmem = pl.BlockSpec(memory_space=pltpu.VMEM)
    dma = pltpu.SemaphoreType.DMA
    return pl.pallas_call(
        functools.partial(layer_kernel, span, kv_count, share, devices, ranks),
        out_shape=jax.ShapeDtypeStruct((rows, features), jnp.bfloat16),
        in_specs=[
            pl.BlockSpec(memory_space=pltpu.SMEM),
            vmem,
            vmem,
            pl.BlockSpec(memory_space=pl.ANY),
        ],
        out_specs=vmem,
        scratch_shapes=[
            pltpu.VMEM((rows * devices, key_value.shape[1]), jnp.bfloat16),
            pltpu.VMEM(key_value.shape, jnp.bfloat16),
            pltpu.VMEM((local_heads, rows, HEAD_DIM), jnp.bfloat16),
            pltpu.VMEM((local_heads, rows, HEAD_DIM), jnp.float32),
            pltpu.VMEM((local_heads, rows, 128), jnp.float32),
            pltpu.VMEM((local_heads, rows, span), jnp.float32),
            pltpu.VMEM((local_heads, rows, span), jnp.bfloat16),
            pltpu.VMEM((span, span), jnp.bfloat16),
            pltpu.VMEM((ranks, rows, width), jnp.bfloat16),
            pltpu.VMEM((ranks, width, features), jnp.bfloat16),
            dma((devices,)),
            dma,
            dma((devices,)),
            dma((devices,)),
            dma((devices,)),
            dma((3,)),
            dma((ranks,)),
            dma((ranks,)),
            dma,
            dma((ranks,)),
            dma((ranks,)),
        ],
        compiler_params=pltpu.CompilerParams(has_side_effects=True),
    )(head_bias, queries, key_value, output_weight)


def solution(mesh):
    placed = (P("sp", None), P(), P(None, "tp"), P(), P(), P("tp"), P("tp", None))
    return jax.shard_map(
        local, mesh=mesh, in_specs=placed, out_specs=P("sp", None), check_vma=False
    )
```

```python
import functools
import math

import jax
import jax.numpy as jnp
from jax import lax
from jax.experimental import pallas as pl
from jax.experimental.pallas import tpu as pltpu
from jax.sharding import PartitionSpec as P

HEADS = 16
KV_HEADS = 4
HEAD_DIM = 64
LOG2E = math.log2(math.e)


PLANE = 4
PACE = 2
ROWS = 192
LAG = 8
MESH = pl.DeviceIdType.MESH


def layer_kernel(
    span, kv_count, share, devices, ranks,
    bias_ref, normed_ref, qw_ref, kv_ref, mix_ref, out_ref,
    pairs, spare, heads_q, total, kept, gain, lost, tri, gathered, mixers,
    arrive, spare_arrive, up_sem, side_sem, over_sem, own_sem, mix_send, mix_arrive, mix_local, att_send, att_arrive,
):
    rows = normed_ref.shape[0]
    heads = kv_count * share
    kv_width = kv_count * HEAD_DIM
    me = lax.axis_index("sp")
    rank = lax.axis_index("tp")
    levels = devices // PLANE
    level = me // PLANE
    place = me % PLANE
    across = PLANE - 1 - place
    side = place + 1 - 2 * (place % 2)
    over = (place + 2) % PLANE
    has_up = level < levels - 1
    offset = me * rows

    def slot(block):
        return pairs.at[pl.ds(pl.multiple_of(block * rows, 16), rows), :]

    def ship(source, block, send, target):
        return pltpu.make_async_remote_copy(
            src_ref=source, dst_ref=slot(block), send_sem=send, recv_sem=arrive.at[block],
            device_id={"sp": target}, device_id_type=MESH,
        )

    def own_to(index, where):
        return ship(kv_ref, me, own_sem.at[index], level * PLANE + where)

    def own_spare():
        return pltpu.make_async_remote_copy(
            src_ref=kv_ref, dst_ref=spare, send_sem=own_sem.at[2], recv_sem=spare_arrive,
            device_id={"sp": level * PLANE + across}, device_id_type=MESH,
        )

    def lift_up():
        return ship(spare, level * PLANE + across, up_sem.at[level * PLANE + across], me + PLANE)

    def own_up():
        return ship(kv_ref, me, up_sem.at[me], me + PLANE)

    def send_up(block):
        return ship(slot(block), block, up_sem.at[block], me + PLANE)

    def send_side(block):
        return ship(slot(block), block, side_sem.at[block], level * PLANE + side)

    def send_over(block):
        return ship(slot(block), block, over_sem.at[block], level * PLANE + over)

    def mixer(step):
        return pltpu.make_async_remote_copy(
            src_ref=mix_ref, dst_ref=mixers.at[rank], send_sem=mix_send.at[step],
            recv_sem=mix_arrive.at[step], device_id={"tp": (rank + step) % ranks}, device_id_type=MESH,
        )

    def attended(step):
        return pltpu.make_async_remote_copy(
            src_ref=gathered.at[rank], dst_ref=gathered.at[rank], send_sem=att_send.at[step],
            recv_sem=att_arrive.at[step], device_id={"tp": (rank + step) % ranks}, device_id_type=MESH,
        )

    barrier = pltpu.get_barrier_semaphore()

    def greet(**where):
        pl.semaphore_signal(barrier, inc=1, device_id=where, device_id_type=MESH)

    for where in (side, over, across):
        greet(sp=level * PLANE + where)
    for step in range(1, ranks):
        greet(tp=(rank + step) % ranks)
    pl.when(has_up)(lambda: greet(sp=me + PLANE))
    pl.when(level > 0)(lambda: greet(sp=me - PLANE))
    pl.semaphore_wait(
        barrier, 2 + ranks + jnp.minimum(level, 1) + jnp.minimum(levels - 1 - level, 1)
    )

    pl.when(has_up)(lambda: own_up().start())
    pl.when((across > place) & has_up)(lambda: own_to(2, across).start())
    pl.when((across < place) & has_up)(lambda: own_spare().start())
    pl.when(side > place)(lambda: own_to(0, side).start())
    pl.when(over > place)(lambda: own_to(1, over).start())
    pl.when((across > place) & (level == levels - 1))(lambda: own_to(2, across).start())
    mine = pltpu.make_async_copy(mix_ref, mixers.at[rank], mix_local)
    mine.start()
    for step in range(1, ranks):
        mixer(step).start()

    pairs[pl.ds(pl.multiple_of(offset, 16), rows), :] = kv_ref[...]
    queries = jnp.dot(normed_ref[...], qw_ref[...], preferred_element_type=jnp.float32)
    queries = queries.astype(jnp.bfloat16)
    for h in range(heads):
        heads_q[h] = queries[:, h * HEAD_DIM : (h + 1) * HEAD_DIM]
    total[...] = jnp.zeros_like(total)
    kept[...] = jnp.zeros_like(kept)
    first_pos = lax.broadcasted_iota(jnp.int32, (span, span), 0)
    second_pos = lax.broadcasted_iota(jnp.int32, (span, span), 1)
    tri[...] = (first_pos > second_pos).astype(jnp.float32).astype(jnp.bfloat16)

    def arrived(block):
        ship(slot(block), block, up_sem.at[block], (me + 1) % devices).wait_recv()

    def relay_column(block):
        arrived(block)
        pl.when(has_up)(lambda: send_up(block).start())
        send_side(block).start()
        send_over(block).start()

    def relay_across(block):
        arrived(block)
        pl.when(has_up)(lambda: send_up(block).start())

    def lift():
        own_spare().wait_recv()
        lift_up().start()

    def relay(group):
        lower = level - group
        held = lower * PLANE + across
        pl.when(lower >= 1)(lambda: relay_column((lower - 1) * PLANE + place))
        pl.when((group == 0) & has_up & (across > place))(lift)
        pl.when((group > 0) | (across < place))(lambda: relay_across(held))

    def relay_until(done, count):
        count = jnp.minimum(count, level + 1)
        ahead = jnp.maximum(count - done, 0)

        def one(index, _):
            relay(done + index)
            return 0

        lax.fori_loop(0, ahead, one, 0)
        return done + ahead

    def take_until(front, low):
        count = jnp.maximum(front - low, 0)

        def one(index, _):
            block = front - 1 - index
            spot = block % PLANE
            pl.when((spot != place) & (spot != across))(lambda: arrived(block))
            return 0

        lax.fori_loop(0, count, one, 0)
        return front - count

    def advance(state, start, turn):
        done, front = state
        low = start // rows
        done = relay_until(done, jnp.maximum(turn // PACE + 1, level - low // PLANE + 1))
        return done, take_until(front, low)

    def chunk(start, masked):
        start = pl.multiple_of(start, span)
        block = pairs[pl.ds(start, span), :]
        if masked:
            key_pos = start + lax.broadcasted_iota(jnp.int32, (rows, span), 1)
            query_pos = offset + lax.broadcasted_iota(jnp.int32, (rows, span), 0)
            strict = key_pos < query_pos
            value_pos = start + lax.broadcasted_iota(jnp.int32, (span, block.shape[1]), 0)
            block = jnp.where(value_pos < offset + rows, block.astype(jnp.float32), 0.0)
            block = block.astype(jnp.bfloat16)
        later = tri[...]
        scale = HEAD_DIM ** (-0.5) * LOG2E
        tiles = [(h, t) for h in range(heads) for t in range(0, rows, ROWS)]

        def first(h, t):
            g = h // share
            dots = lax.dot_general(
                heads_q[h, t : t + ROWS], block[:, g * HEAD_DIM : (g + 1) * HEAD_DIM],
                (((1,), (1,)), ((), ())), preferred_element_type=jnp.float32,
            )
            u = dots * scale + bias_ref[h] * LOG2E
            drop = jnp.maximum(u, jnp.log2(1.0 + jnp.exp2(jnp.minimum(u, 126.0))))
            if masked:
                drop = jnp.where(strict[t : t + ROWS], drop, 0.0)
            gain[h, t : t + ROWS] = u - drop
            lost[h, t : t + ROWS] = drop.astype(jnp.bfloat16)
            return drop[:, :1]

        def second(h, t, head):
            g = h // share
            part = slice(t, t + ROWS)
            after = jnp.dot(lost[h, part], later, preferred_element_type=jnp.float32)
            weight = jnp.exp2(gain[h, part] - (after + jnp.tile(kept[h, part], (1, span // 128))))
            if masked:
                weight = jnp.where(strict[part], weight, 0.0)
            kept[h, part] += jnp.broadcast_to(after[:, :1] + head, (ROWS, 128))
            total[h, part] += jnp.dot(
                weight.astype(jnp.bfloat16),
                block[:, kv_width + g * HEAD_DIM : kv_width + (g + 1) * HEAD_DIM],
                preferred_element_type=jnp.float32,
            )

        waiting = []
        for h, t in tiles:
            waiting.append((h, t, first(h, t)))
            if len(waiting) > LAG:
                second(*waiting.pop(0))
        for item in waiting:
            second(*item)

    whole = offset // span
    turns = (offset + rows + span - 1) // span

    def edge(turn, state):
        start = (turns - 1 - turn) * span
        state = advance(state, start, turn)
        chunk(start, True)
        return state

    def plain(turn, state):
        start = (whole - 1 - turn) * span
        state = advance(state, start, turn + turns - whole)
        chunk(start, False)
        return state

    state = lax.fori_loop(0, turns - whole, edge, (0, me))
    done, front = lax.fori_loop(0, whole, plain, state)
    relay_until(done, level + 1)
    take_until(front, 0)

    for h in range(heads):
        gathered[rank, :, h * HEAD_DIM : (h + 1) * HEAD_DIM] = total[h].astype(jnp.bfloat16)
    for step in range(1, ranks):
        attended(step).start()
    mine.wait()
    for step in range(1, ranks):
        mixer(step).wait_recv()
    for step in range(1, ranks):
        attended(step).wait_recv()
    features = out_ref.shape[1]
    tile = math.gcd(features, 512)
    for column in range(0, features, tile):
        summed = jnp.zeros((rows, tile), jnp.float32)
        for r in range(ranks):
            summed += jnp.dot(
                gathered[r], mixers[r, :, column : column + tile], preferred_element_type=jnp.float32
            )
        out_ref[:, column : column + tile] = summed.astype(jnp.bfloat16)

    pl.when(side > place)(lambda: own_to(0, side).wait_send())
    pl.when(over > place)(lambda: own_to(1, over).wait_send())
    pl.when(across > place)(lambda: own_to(2, across).wait_send())
    pl.when((across < place) & has_up)(lambda: own_spare().wait_send())
    pl.when(has_up)(lambda: own_up().wait_send())
    pl.when(has_up & (across > place))(lambda: lift_up().wait_send())

    def settle(block, _):
        spot = block % PLANE
        lower = block // PLANE < level

        def plane_done():
            send_side(block).wait_send()
            send_over(block).wait_send()

        pl.when(has_up & ((spot == place) | (spot == across)))(lambda: send_up(block).wait_send())
        pl.when(lower & (spot == place))(plane_done)
        return 0

    lax.fori_loop(0, me, settle, 0)
    for step in range(1, ranks):
        mixer(step).wait_send()
        attended(step).wait_send()


def local(hidden, norm_gain, query_weight, key_weight, value_weight, head_bias, output_weight):
    group = HEADS // KV_HEADS
    local_heads = query_weight.shape[1] // HEAD_DIM
    kv_count = max(1, local_heads // group)
    share = min(local_heads, group)
    first = lax.axis_index("tp") * local_heads // group
    key_cols = lax.dynamic_slice_in_dim(key_weight, first * HEAD_DIM, kv_count * HEAD_DIM, 1)
    value_cols = lax.dynamic_slice_in_dim(value_weight, first * HEAD_DIM, kv_count * HEAD_DIM, 1)
    wide = hidden.astype(jnp.float32)
    normed = (
        wide * lax.rsqrt(jnp.mean(wide * wide, axis=-1, keepdims=True) + 1e-06) * norm_gain
    ).astype(jnp.bfloat16)
    joined = jnp.concatenate([key_cols, value_cols], axis=1)
    key_value = jnp.dot(normed, joined, preferred_element_type=jnp.float32).astype(jnp.bfloat16)
    rows = normed.shape[0]
    devices = lax.axis_size("sp")
    ranks = lax.axis_size("tp")
    span = math.gcd(rows * devices, 256)
    width = query_weight.shape[1]
    features = output_weight.shape[1]
    vmem = pl.BlockSpec(memory_space=pltpu.VMEM)
    dma = pltpu.SemaphoreType.DMA
    return pl.pallas_call(
        functools.partial(layer_kernel, span, kv_count, share, devices, ranks),
        out_shape=jax.ShapeDtypeStruct((rows, features), jnp.bfloat16),
        in_specs=[
            pl.BlockSpec(memory_space=pltpu.SMEM),
            vmem,
            vmem,
            vmem,
            pl.BlockSpec(memory_space=pl.ANY),
        ],
        out_specs=vmem,
        scratch_shapes=[
            pltpu.VMEM((rows * devices, key_value.shape[1]), jnp.bfloat16),
            pltpu.VMEM(key_value.shape, jnp.bfloat16),
            pltpu.VMEM((local_heads, rows, HEAD_DIM), jnp.bfloat16),
            pltpu.VMEM((local_heads, rows, HEAD_DIM), jnp.float32),
            pltpu.VMEM((local_heads, rows, 128), jnp.float32),
            pltpu.VMEM((local_heads, rows, span), jnp.float32),
            pltpu.VMEM((local_heads, rows, span), jnp.bfloat16),
            pltpu.VMEM((span, span), jnp.bfloat16),
            pltpu.VMEM((ranks, rows, width), jnp.bfloat16),
            pltpu.VMEM((ranks, width, features), jnp.bfloat16),
            dma((devices,)),
            dma,
            dma((devices,)),
            dma((devices,)),
            dma((devices,)),
            dma((3,)),
            dma((ranks,)),
            dma((ranks,)),
            dma,
            dma((ranks,)),
            dma((ranks,)),
        ],
        compiler_params=pltpu.CompilerParams(has_side_effects=True, collective_id=0),
    )(head_bias, normed, query_weight, key_value, output_weight)


def solution(mesh):
    placed = (P("sp", None), P(), P(None, "tp"), P(), P(), P("tp"), P("tp", None))
    return jax.shard_map(
        local, mesh=mesh, in_specs=placed, out_specs=P("sp", None), check_vma=False
    )
```

```python
import functools
import math

import jax
import jax.numpy as jnp
from jax import lax
from jax.experimental import pallas as pl
from jax.experimental.pallas import tpu as pltpu
from jax.sharding import PartitionSpec as P

HEADS = 16
KV_HEADS = 4
HEAD_DIM = 64
LOG2E = math.log2(math.e)


PLANE = 4
PACE = 2
ROWS = 192
LAG = 8
MESH = pl.DeviceIdType.MESH


def layer_kernel(
    span, kv_count, share, devices, ranks,
    bias_ref, hidden_ref, gain_ref, qw_ref, kvw_ref, mix_ref, out_ref,
    pairs, spare, normed_ref, kv_ref, heads_q, total, kept, gain, lost, tri, gathered, mixers,
    arrive, spare_arrive, up_sem, side_sem, over_sem, own_sem, mix_send, mix_arrive, mix_local, att_send, att_arrive,
):
    rows = hidden_ref.shape[0]
    heads = kv_count * share
    kv_width = kv_count * HEAD_DIM
    me = lax.axis_index("sp")
    rank = lax.axis_index("tp")
    levels = devices // PLANE
    level = me // PLANE
    place = me % PLANE
    across = PLANE - 1 - place
    side = place + 1 - 2 * (place % 2)
    over = (place + 2) % PLANE
    has_up = level < levels - 1
    offset = me * rows

    def slot(block):
        return pairs.at[pl.ds(pl.multiple_of(block * rows, 16), rows), :]

    def ship(source, block, send, target):
        return pltpu.make_async_remote_copy(
            src_ref=source, dst_ref=slot(block), send_sem=send, recv_sem=arrive.at[block],
            device_id={"sp": target}, device_id_type=MESH,
        )

    def own_to(index, where):
        return ship(kv_ref, me, own_sem.at[index], level * PLANE + where)

    def own_spare():
        return pltpu.make_async_remote_copy(
            src_ref=kv_ref, dst_ref=spare, send_sem=own_sem.at[2], recv_sem=spare_arrive,
            device_id={"sp": level * PLANE + across}, device_id_type=MESH,
        )

    def lift_up():
        return ship(spare, level * PLANE + across, up_sem.at[level * PLANE + across], me + PLANE)

    def own_up():
        return ship(kv_ref, me, up_sem.at[me], me + PLANE)

    def send_up(block):
        return ship(slot(block), block, up_sem.at[block], me + PLANE)

    def send_side(block):
        return ship(slot(block), block, side_sem.at[block], level * PLANE + side)

    def send_over(block):
        return ship(slot(block), block, over_sem.at[block], level * PLANE + over)

    def mixer(step):
        return pltpu.make_async_remote_copy(
            src_ref=mix_ref, dst_ref=mixers.at[rank], send_sem=mix_send.at[step],
            recv_sem=mix_arrive.at[step], device_id={"tp": (rank + step) % ranks}, device_id_type=MESH,
        )

    def attended(step):
        return pltpu.make_async_remote_copy(
            src_ref=gathered.at[rank], dst_ref=gathered.at[rank], send_sem=att_send.at[step],
            recv_sem=att_arrive.at[step], device_id={"tp": (rank + step) % ranks}, device_id_type=MESH,
        )

    barrier = pltpu.get_barrier_semaphore()

    def greet(**where):
        pl.semaphore_signal(barrier, inc=1, device_id=where, device_id_type=MESH)

    for where in (side, over, across):
        greet(sp=level * PLANE + where)
    for step in range(1, ranks):
        greet(tp=(rank + step) % ranks)
    pl.when(has_up)(lambda: greet(sp=me + PLANE))
    pl.when(level > 0)(lambda: greet(sp=me - PLANE))
    wide = hidden_ref[...].astype(jnp.float32)
    normed = wide * lax.rsqrt(jnp.mean(wide * wide, axis=-1, keepdims=True) + 1e-06) * gain_ref[...]
    normed_ref[...] = normed.astype(jnp.bfloat16)
    key_value = jnp.dot(normed_ref[...], kvw_ref[...], preferred_element_type=jnp.float32)
    key_value = key_value.astype(jnp.bfloat16)
    kv_ref[...] = key_value
    pairs[pl.ds(pl.multiple_of(offset, 16), rows), :] = key_value
    pl.semaphore_wait(
        barrier, 2 + ranks + jnp.minimum(level, 1) + jnp.minimum(levels - 1 - level, 1)
    )

    pl.when(has_up)(lambda: own_up().start())
    pl.when((across > place) & has_up)(lambda: own_to(2, across).start())
    pl.when((across < place) & has_up)(lambda: own_spare().start())
    pl.when(side > place)(lambda: own_to(0, side).start())
    pl.when(over > place)(lambda: own_to(1, over).start())
    pl.when((across > place) & (level == levels - 1))(lambda: own_to(2, across).start())
    mine = pltpu.make_async_copy(mix_ref, mixers.at[rank], mix_local)
    mine.start()
    for step in range(1, ranks):
        mixer(step).start()

    queries = jnp.dot(normed_ref[...], qw_ref[...], preferred_element_type=jnp.float32)
    queries = queries.astype(jnp.bfloat16)
    for h in range(heads):
        heads_q[h] = queries[:, h * HEAD_DIM : (h + 1) * HEAD_DIM]
    total[...] = jnp.zeros_like(total)
    kept[...] = jnp.zeros_like(kept)
    first_pos = lax.broadcasted_iota(jnp.int32, (span, span), 0)
    second_pos = lax.broadcasted_iota(jnp.int32, (span, span), 1)
    tri[...] = (first_pos > second_pos).astype(jnp.float32).astype(jnp.bfloat16)

    def arrived(block):
        ship(slot(block), block, up_sem.at[block], (me + 1) % devices).wait_recv()

    def relay_column(block):
        arrived(block)
        pl.when(has_up)(lambda: send_up(block).start())
        send_side(block).start()
        send_over(block).start()

    def relay_across(block):
        arrived(block)
        pl.when(has_up)(lambda: send_up(block).start())

    def lift():
        own_spare().wait_recv()
        lift_up().start()

    def relay(group):
        lower = level - group
        held = lower * PLANE + across
        pl.when(lower >= 1)(lambda: relay_column((lower - 1) * PLANE + place))
        pl.when((group == 0) & has_up & (across > place))(lift)
        pl.when((group > 0) | (across < place))(lambda: relay_across(held))

    def relay_until(done, count):
        count = jnp.minimum(count, level + 1)
        ahead = jnp.maximum(count - done, 0)

        def one(index, _):
            relay(done + index)
            return 0

        lax.fori_loop(0, ahead, one, 0)
        return done + ahead

    def take_until(front, low):
        count = jnp.maximum(front - low, 0)

        def one(index, _):
            block = front - 1 - index
            spot = block % PLANE
            pl.when((spot != place) & (spot != across))(lambda: arrived(block))
            return 0

        lax.fori_loop(0, count, one, 0)
        return front - count

    def advance(state, start, turn):
        done, front = state
        low = start // rows
        done = relay_until(done, jnp.maximum(turn // PACE + 1, level - low // PLANE + 1))
        return done, take_until(front, low)

    def chunk(start, masked):
        start = pl.multiple_of(start, span)
        block = pairs[pl.ds(start, span), :]
        if masked:
            key_pos = start + lax.broadcasted_iota(jnp.int32, (rows, span), 1)
            query_pos = offset + lax.broadcasted_iota(jnp.int32, (rows, span), 0)
            strict = key_pos < query_pos
            value_pos = start + lax.broadcasted_iota(jnp.int32, (span, block.shape[1]), 0)
            block = jnp.where(value_pos < offset + rows, block.astype(jnp.float32), 0.0)
            block = block.astype(jnp.bfloat16)
        later = tri[...]
        scale = HEAD_DIM ** (-0.5) * LOG2E
        tiles = [(h, t) for h in range(heads) for t in range(0, rows, ROWS)]

        def first(h, t):
            g = h // share
            dots = lax.dot_general(
                heads_q[h, t : t + ROWS], block[:, g * HEAD_DIM : (g + 1) * HEAD_DIM],
                (((1,), (1,)), ((), ())), preferred_element_type=jnp.float32,
            )
            u = dots * scale + bias_ref[h] * LOG2E
            drop = jnp.maximum(u, jnp.log2(1.0 + jnp.exp2(jnp.minimum(u, 126.0))))
            if masked:
                drop = jnp.where(strict[t : t + ROWS], drop, 0.0)
            gain[h, t : t + ROWS] = u - drop
            lost[h, t : t + ROWS] = drop.astype(jnp.bfloat16)
            return drop[:, :1]

        def second(h, t, head):
            g = h // share
            part = slice(t, t + ROWS)
            after = jnp.dot(lost[h, part], later, preferred_element_type=jnp.float32)
            weight = jnp.exp2(gain[h, part] - (after + jnp.tile(kept[h, part], (1, span // 128))))
            if masked:
                weight = jnp.where(strict[part], weight, 0.0)
            kept[h, part] += jnp.broadcast_to(after[:, :1] + head, (ROWS, 128))
            total[h, part] += jnp.dot(
                weight.astype(jnp.bfloat16),
                block[:, kv_width + g * HEAD_DIM : kv_width + (g + 1) * HEAD_DIM],
                preferred_element_type=jnp.float32,
            )

        waiting = []
        for h, t in tiles:
            waiting.append((h, t, first(h, t)))
            if len(waiting) > LAG:
                second(*waiting.pop(0))
        for item in waiting:
            second(*item)

    whole = offset // span
    turns = (offset + rows + span - 1) // span

    def edge(turn, state):
        start = (turns - 1 - turn) * span
        state = advance(state, start, turn)
        chunk(start, True)
        return state

    def plain(turn, state):
        start = (whole - 1 - turn) * span
        state = advance(state, start, turn + turns - whole)
        chunk(start, False)
        return state

    state = lax.fori_loop(0, turns - whole, edge, (0, me))
    done, front = lax.fori_loop(0, whole, plain, state)
    relay_until(done, level + 1)
    take_until(front, 0)

    for h in range(heads):
        gathered[rank, :, h * HEAD_DIM : (h + 1) * HEAD_DIM] = total[h].astype(jnp.bfloat16)
    for step in range(1, ranks):
        attended(step).start()
    mine.wait()
    for step in range(1, ranks):
        mixer(step).wait_recv()
    for step in range(1, ranks):
        attended(step).wait_recv()
    features = out_ref.shape[1]
    tile = math.gcd(features, 512)
    for column in range(0, features, tile):
        summed = jnp.zeros((rows, tile), jnp.float32)
        for r in range(ranks):
            summed += jnp.dot(
                gathered[r], mixers[r, :, column : column + tile], preferred_element_type=jnp.float32
            )
        out_ref[:, column : column + tile] = summed.astype(jnp.bfloat16)

    pl.when(side > place)(lambda: own_to(0, side).wait_send())
    pl.when(over > place)(lambda: own_to(1, over).wait_send())
    pl.when(across > place)(lambda: own_to(2, across).wait_send())
    pl.when((across < place) & has_up)(lambda: own_spare().wait_send())
    pl.when(has_up)(lambda: own_up().wait_send())
    pl.when(has_up & (across > place))(lambda: lift_up().wait_send())

    def settle(block, _):
        spot = block % PLANE
        lower = block // PLANE < level

        def plane_done():
            send_side(block).wait_send()
            send_over(block).wait_send()

        pl.when(has_up & ((spot == place) | (spot == across)))(lambda: send_up(block).wait_send())
        pl.when(lower & (spot == place))(plane_done)
        return 0

    lax.fori_loop(0, me, settle, 0)
    for step in range(1, ranks):
        mixer(step).wait_send()
        attended(step).wait_send()


def local(hidden, norm_gain, query_weight, key_weight, value_weight, head_bias, output_weight):
    group = HEADS // KV_HEADS
    local_heads = query_weight.shape[1] // HEAD_DIM
    kv_count = max(1, local_heads // group)
    share = min(local_heads, group)
    first = lax.axis_index("tp") * local_heads // group
    key_cols = lax.dynamic_slice_in_dim(key_weight, first * HEAD_DIM, kv_count * HEAD_DIM, 1)
    value_cols = lax.dynamic_slice_in_dim(value_weight, first * HEAD_DIM, kv_count * HEAD_DIM, 1)
    joined = jnp.concatenate([key_cols, value_cols], axis=1)
    rows = hidden.shape[0]
    devices = lax.axis_size("sp")
    ranks = lax.axis_size("tp")
    span = math.gcd(rows * devices, 256)
    width = query_weight.shape[1]
    features = output_weight.shape[1]
    vmem = pl.BlockSpec(memory_space=pltpu.VMEM)
    dma = pltpu.SemaphoreType.DMA
    return pl.pallas_call(
        functools.partial(layer_kernel, span, kv_count, share, devices, ranks),
        out_shape=jax.ShapeDtypeStruct((rows, features), jnp.bfloat16),
        in_specs=[
            pl.BlockSpec(memory_space=pltpu.SMEM),
            vmem,
            vmem,
            vmem,
            vmem,
            pl.BlockSpec(memory_space=pl.ANY),
        ],
        out_specs=vmem,
        scratch_shapes=[
            pltpu.VMEM((rows * devices, joined.shape[1]), jnp.bfloat16),
            pltpu.VMEM((rows, joined.shape[1]), jnp.bfloat16),
            pltpu.VMEM(hidden.shape, jnp.bfloat16),
            pltpu.VMEM((rows, joined.shape[1]), jnp.bfloat16),
            pltpu.VMEM((local_heads, rows, HEAD_DIM), jnp.bfloat16),
            pltpu.VMEM((local_heads, rows, HEAD_DIM), jnp.float32),
            pltpu.VMEM((local_heads, rows, 128), jnp.float32),
            pltpu.VMEM((local_heads, rows, span), jnp.float32),
            pltpu.VMEM((local_heads, rows, span), jnp.bfloat16),
            pltpu.VMEM((span, span), jnp.bfloat16),
            pltpu.VMEM((ranks, rows, width), jnp.bfloat16),
            pltpu.VMEM((ranks, width, features), jnp.bfloat16),
            dma((devices,)),
            dma,
            dma((devices,)),
            dma((devices,)),
            dma((devices,)),
            dma((3,)),
            dma((ranks,)),
            dma((ranks,)),
            dma,
            dma((ranks,)),
            dma((ranks,)),
        ],
        compiler_params=pltpu.CompilerParams(has_side_effects=True, collective_id=0),
    )(head_bias, hidden, norm_gain[None, :], query_weight, joined, output_weight)


def solution(mesh):
    placed = (P("sp", None), P(), P(None, "tp"), P(), P(), P("tp"), P("tp", None))
    return jax.shard_map(
        local, mesh=mesh, in_specs=placed, out_specs=P("sp", None), check_vma=False
    )
```

```python
import functools
import math

import jax
import jax.numpy as jnp
from jax import lax
from jax.experimental import pallas as pl
from jax.experimental.pallas import tpu as pltpu
from jax.sharding import PartitionSpec as P

HEADS = 16
KV_HEADS = 4
HEAD_DIM = 64
LOG2E = math.log2(math.e)


PLANE = 4
PACE = 2
ROWS = 192
LAG = 8
MESH = pl.DeviceIdType.MESH


def layer_kernel(
    span, kv_count, share, devices, ranks, sliced,
    bias_ref, hidden_ref, gain_ref, qw_hbm, kw_hbm, vw_hbm, mix_ref, out_ref,
    pairs, spare, normed_ref, kv_ref, qw_ref, kvw_ref, heads_q, total, kept, gain, lost, tri, gathered, mixers,
    arrive, spare_arrive, up_sem, side_sem, over_sem, own_sem, mix_send, mix_arrive, mix_local, att_send, att_arrive, load_sem,
):
    rows = hidden_ref.shape[0]
    heads = kv_count * share
    kv_width = kv_count * HEAD_DIM
    me = lax.axis_index("sp")
    rank = lax.axis_index("tp")
    levels = devices // PLANE
    level = me // PLANE
    place = me % PLANE
    across = PLANE - 1 - place
    side = place + 1 - 2 * (place % 2)
    over = (place + 2) % PLANE
    has_up = level < levels - 1
    offset = me * rows

    def slot(block):
        return pairs.at[pl.ds(pl.multiple_of(block * rows, 16), rows), :]

    def ship(source, block, send, target):
        return pltpu.make_async_remote_copy(
            src_ref=source, dst_ref=slot(block), send_sem=send, recv_sem=arrive.at[block],
            device_id={"sp": target}, device_id_type=MESH,
        )

    def own_to(index, where):
        return ship(kv_ref, me, own_sem.at[index], level * PLANE + where)

    def own_spare():
        return pltpu.make_async_remote_copy(
            src_ref=kv_ref, dst_ref=spare, send_sem=own_sem.at[2], recv_sem=spare_arrive,
            device_id={"sp": level * PLANE + across}, device_id_type=MESH,
        )

    def lift_up():
        return ship(spare, level * PLANE + across, up_sem.at[level * PLANE + across], me + PLANE)

    def own_up():
        return ship(kv_ref, me, up_sem.at[me], me + PLANE)

    def send_up(block):
        return ship(slot(block), block, up_sem.at[block], me + PLANE)

    def send_side(block):
        return ship(slot(block), block, side_sem.at[block], level * PLANE + side)

    def send_over(block):
        return ship(slot(block), block, over_sem.at[block], level * PLANE + over)

    def mixer(step):
        return pltpu.make_async_remote_copy(
            src_ref=mix_ref, dst_ref=mixers.at[rank], send_sem=mix_send.at[step],
            recv_sem=mix_arrive.at[step], device_id={"tp": (rank + step) % ranks}, device_id_type=MESH,
        )

    def attended(step):
        return pltpu.make_async_remote_copy(
            src_ref=gathered.at[rank], dst_ref=gathered.at[rank], send_sem=att_send.at[step],
            recv_sem=att_arrive.at[step], device_id={"tp": (rank + step) % ranks}, device_id_type=MESH,
        )

    if sliced:
        column = pl.multiple_of(rank * kv_width, kv_width)
        loads = [
            pltpu.make_async_copy(
                source.at[:, pl.ds(column, kv_width)],
                kvw_ref.at[:, pl.ds(index * kv_width, kv_width)],
                load_sem.at[index],
            )
            for index, source in enumerate((kw_hbm, vw_hbm))
        ]
    else:
        loads = [pltpu.make_async_copy(kw_hbm, kvw_ref, load_sem.at[0])]
    query_load = pltpu.make_async_copy(qw_hbm, qw_ref, load_sem.at[2])
    for load in loads:
        load.start()
    query_load.start()

    barrier = pltpu.get_barrier_semaphore()

    def greet(**where):
        pl.semaphore_signal(barrier, inc=1, device_id=where, device_id_type=MESH)

    for where in (side, over, across):
        greet(sp=level * PLANE + where)
    for step in range(1, ranks):
        greet(tp=(rank + step) % ranks)
    pl.when(has_up)(lambda: greet(sp=me + PLANE))
    pl.when(level > 0)(lambda: greet(sp=me - PLANE))
    wide = hidden_ref[...].astype(jnp.float32)
    normed = wide * lax.rsqrt(jnp.mean(wide * wide, axis=-1, keepdims=True) + 1e-06) * gain_ref[...]
    normed_ref[...] = normed.astype(jnp.bfloat16)
    for load in loads:
        load.wait()
    key_value = jnp.dot(normed_ref[...], kvw_ref[...], preferred_element_type=jnp.float32)
    key_value = key_value.astype(jnp.bfloat16)
    kv_ref[...] = key_value
    pairs[pl.ds(pl.multiple_of(offset, 16), rows), :] = key_value
    pl.semaphore_wait(
        barrier, 2 + ranks + jnp.minimum(level, 1) + jnp.minimum(levels - 1 - level, 1)
    )

    pl.when(has_up)(lambda: own_up().start())
    pl.when((across > place) & has_up)(lambda: own_to(2, across).start())
    pl.when((across < place) & has_up)(lambda: own_spare().start())
    pl.when(side > place)(lambda: own_to(0, side).start())
    pl.when(over > place)(lambda: own_to(1, over).start())
    pl.when((across > place) & (level == levels - 1))(lambda: own_to(2, across).start())
    mine = pltpu.make_async_copy(mix_ref, mixers.at[rank], mix_local)
    mine.start()
    for step in range(1, ranks):
        mixer(step).start()

    query_load.wait()
    queries = jnp.dot(normed_ref[...], qw_ref[...], preferred_element_type=jnp.float32)
    queries = queries.astype(jnp.bfloat16)
    for h in range(heads):
        heads_q[h] = queries[:, h * HEAD_DIM : (h + 1) * HEAD_DIM]
    total[...] = jnp.zeros_like(total)
    kept[...] = jnp.zeros_like(kept)
    first_pos = lax.broadcasted_iota(jnp.int32, (span, span), 0)
    second_pos = lax.broadcasted_iota(jnp.int32, (span, span), 1)
    tri[...] = (first_pos > second_pos).astype(jnp.float32).astype(jnp.bfloat16)

    def arrived(block):
        ship(slot(block), block, up_sem.at[block], (me + 1) % devices).wait_recv()

    def relay_column(block):
        arrived(block)
        pl.when(has_up)(lambda: send_up(block).start())
        send_side(block).start()
        send_over(block).start()

    def relay_across(block):
        arrived(block)
        pl.when(has_up)(lambda: send_up(block).start())

    def lift():
        own_spare().wait_recv()
        lift_up().start()

    def relay(group):
        lower = level - group
        held = lower * PLANE + across
        pl.when(lower >= 1)(lambda: relay_column((lower - 1) * PLANE + place))
        pl.when((group == 0) & has_up & (across > place))(lift)
        pl.when((group > 0) | (across < place))(lambda: relay_across(held))

    def relay_until(done, count):
        count = jnp.minimum(count, level + 1)
        ahead = jnp.maximum(count - done, 0)

        def one(index, _):
            relay(done + index)
            return 0

        lax.fori_loop(0, ahead, one, 0)
        return done + ahead

    def take_until(front, low):
        count = jnp.maximum(front - low, 0)

        def one(index, _):
            block = front - 1 - index
            spot = block % PLANE
            pl.when((spot != place) & (spot != across))(lambda: arrived(block))
            return 0

        lax.fori_loop(0, count, one, 0)
        return front - count

    def advance(state, start, turn):
        done, front = state
        low = start // rows
        done = relay_until(done, jnp.maximum(turn // PACE + 1, level - low // PLANE + 1))
        return done, take_until(front, low)

    def chunk(start, masked):
        start = pl.multiple_of(start, span)
        block = pairs[pl.ds(start, span), :]
        if masked:
            key_pos = start + lax.broadcasted_iota(jnp.int32, (rows, span), 1)
            query_pos = offset + lax.broadcasted_iota(jnp.int32, (rows, span), 0)
            strict = key_pos < query_pos
            value_pos = start + lax.broadcasted_iota(jnp.int32, (span, block.shape[1]), 0)
            block = jnp.where(value_pos < offset + rows, block.astype(jnp.float32), 0.0)
            block = block.astype(jnp.bfloat16)
        later = tri[...]
        scale = HEAD_DIM ** (-0.5) * LOG2E
        tiles = [(h, t) for h in range(heads) for t in range(0, rows, ROWS)]

        def first(h, t):
            g = h // share
            dots = lax.dot_general(
                heads_q[h, t : t + ROWS], block[:, g * HEAD_DIM : (g + 1) * HEAD_DIM],
                (((1,), (1,)), ((), ())), preferred_element_type=jnp.float32,
            )
            u = dots * scale + bias_ref[h] * LOG2E
            drop = jnp.maximum(u, jnp.log2(1.0 + jnp.exp2(jnp.minimum(u, 126.0))))
            if masked:
                drop = jnp.where(strict[t : t + ROWS], drop, 0.0)
            gain[h, t : t + ROWS] = u - drop
            lost[h, t : t + ROWS] = drop.astype(jnp.bfloat16)
            return drop[:, :1]

        def second(h, t, head):
            g = h // share
            part = slice(t, t + ROWS)
            after = jnp.dot(lost[h, part], later, preferred_element_type=jnp.float32)
            weight = jnp.exp2(gain[h, part] - (after + jnp.tile(kept[h, part], (1, span // 128))))
            if masked:
                weight = jnp.where(strict[part], weight, 0.0)
            kept[h, part] += jnp.broadcast_to(after[:, :1] + head, (ROWS, 128))
            total[h, part] += jnp.dot(
                weight.astype(jnp.bfloat16),
                block[:, kv_width + g * HEAD_DIM : kv_width + (g + 1) * HEAD_DIM],
                preferred_element_type=jnp.float32,
            )

        waiting = []
        for h, t in tiles:
            waiting.append((h, t, first(h, t)))
            if len(waiting) > LAG:
                second(*waiting.pop(0))
        for item in waiting:
            second(*item)

    whole = offset // span
    turns = (offset + rows + span - 1) // span

    def edge(turn, state):
        start = (turns - 1 - turn) * span
        state = advance(state, start, turn)
        chunk(start, True)
        return state

    def plain(turn, state):
        start = (whole - 1 - turn) * span
        state = advance(state, start, turn + turns - whole)
        chunk(start, False)
        return state

    state = lax.fori_loop(0, turns - whole, edge, (0, me))
    done, front = lax.fori_loop(0, whole, plain, state)
    relay_until(done, level + 1)
    take_until(front, 0)

    for h in range(heads):
        gathered[rank, :, h * HEAD_DIM : (h + 1) * HEAD_DIM] = total[h].astype(jnp.bfloat16)
    for step in range(1, ranks):
        attended(step).start()
    mine.wait()
    for step in range(1, ranks):
        mixer(step).wait_recv()
    for step in range(1, ranks):
        attended(step).wait_recv()
    features = out_ref.shape[1]
    tile = math.gcd(features, 512)
    for column in range(0, features, tile):
        summed = jnp.zeros((rows, tile), jnp.float32)
        for r in range(ranks):
            summed += jnp.dot(
                gathered[r], mixers[r, :, column : column + tile], preferred_element_type=jnp.float32
            )
        out_ref[:, column : column + tile] = summed.astype(jnp.bfloat16)

    pl.when(side > place)(lambda: own_to(0, side).wait_send())
    pl.when(over > place)(lambda: own_to(1, over).wait_send())
    pl.when(across > place)(lambda: own_to(2, across).wait_send())
    pl.when((across < place) & has_up)(lambda: own_spare().wait_send())
    pl.when(has_up)(lambda: own_up().wait_send())
    pl.when(has_up & (across > place))(lambda: lift_up().wait_send())

    def settle(block, _):
        spot = block % PLANE
        lower = block // PLANE < level

        def plane_done():
            send_side(block).wait_send()
            send_over(block).wait_send()

        pl.when(has_up & ((spot == place) | (spot == across)))(lambda: send_up(block).wait_send())
        pl.when(lower & (spot == place))(plane_done)
        return 0

    lax.fori_loop(0, me, settle, 0)
    for step in range(1, ranks):
        mixer(step).wait_send()
        attended(step).wait_send()


def local(hidden, norm_gain, query_weight, key_weight, value_weight, head_bias, output_weight):
    group = HEADS // KV_HEADS
    local_heads = query_weight.shape[1] // HEAD_DIM
    kv_count = max(1, local_heads // group)
    share = min(local_heads, group)
    kv_width = kv_count * HEAD_DIM
    sliced = kv_width % 128 == 0 and local_heads % group == 0
    if sliced:
        key_side, value_side = key_weight, value_weight
    else:
        first = lax.axis_index("tp") * local_heads // group
        key_cols = lax.dynamic_slice_in_dim(key_weight, first * HEAD_DIM, kv_width, 1)
        value_cols = lax.dynamic_slice_in_dim(value_weight, first * HEAD_DIM, kv_width, 1)
        key_side = value_side = jnp.concatenate([key_cols, value_cols], axis=1)
    rows = hidden.shape[0]
    devices = lax.axis_size("sp")
    ranks = lax.axis_size("tp")
    span = math.gcd(rows * devices, 256)
    width = query_weight.shape[1]
    features = output_weight.shape[1]
    vmem = pl.BlockSpec(memory_space=pltpu.VMEM)
    hbm = pl.BlockSpec(memory_space=pl.ANY)
    dma = pltpu.SemaphoreType.DMA
    return pl.pallas_call(
        functools.partial(layer_kernel, span, kv_count, share, devices, ranks, sliced),
        out_shape=jax.ShapeDtypeStruct((rows, features), jnp.bfloat16),
        in_specs=[
            pl.BlockSpec(memory_space=pltpu.SMEM),
            vmem,
            vmem,
            hbm,
            hbm,
            hbm,
            hbm,
        ],
        out_specs=vmem,
        scratch_shapes=[
            pltpu.VMEM((rows * devices, 2 * kv_width), jnp.bfloat16),
            pltpu.VMEM((rows, 2 * kv_width), jnp.bfloat16),
            pltpu.VMEM(hidden.shape, jnp.bfloat16),
            pltpu.VMEM((rows, 2 * kv_width), jnp.bfloat16),
            pltpu.VMEM(query_weight.shape, jnp.bfloat16),
            pltpu.VMEM((query_weight.shape[0], 2 * kv_width), jnp.bfloat16),
            pltpu.VMEM((local_heads, rows, HEAD_DIM), jnp.bfloat16),
            pltpu.VMEM((local_heads, rows, HEAD_DIM), jnp.float32),
            pltpu.VMEM((local_heads, rows, 128), jnp.float32),
            pltpu.VMEM((local_heads, rows, span), jnp.float32),
            pltpu.VMEM((local_heads, rows, span), jnp.bfloat16),
            pltpu.VMEM((span, span), jnp.bfloat16),
            pltpu.VMEM((ranks, rows, width), jnp.bfloat16),
            pltpu.VMEM((ranks, width, features), jnp.bfloat16),
            dma((devices,)),
            dma,
            dma((devices,)),
            dma((devices,)),
            dma((devices,)),
            dma((3,)),
            dma((ranks,)),
            dma((ranks,)),
            dma,
            dma((ranks,)),
            dma((ranks,)),
            dma((3,)),
        ],
        compiler_params=pltpu.CompilerParams(has_side_effects=True, collective_id=0),
    )(head_bias, hidden, norm_gain[None, :], query_weight, key_side, value_side, output_weight)


def solution(mesh):
    placed = (P("sp", None), P(), P(None, "tp"), P(), P(), P("tp"), P("tp", None))
    return jax.shard_map(
        local, mesh=mesh, in_specs=placed, out_specs=P("sp", None), check_vma=False
    )
```

```python
import functools
import math

import jax
import jax.numpy as jnp
from jax import lax
from jax.experimental import pallas as pl
from jax.experimental.pallas import tpu as pltpu
from jax.sharding import PartitionSpec as P

HEADS = 16
KV_HEADS = 4
HEAD_DIM = 64
LOG2E = math.log2(math.e)


PLANE = 4
PACE = 3
ROWS = 192
LAG = 8
MESH = pl.DeviceIdType.MESH


def layer_kernel(
    span, kv_count, share, devices, ranks, sliced,
    bias_ref, hidden_ref, gain_ref, qw_hbm, kw_hbm, vw_hbm, mix_ref, out_ref,
    pairs, spare, normed_ref, kv_ref, qw_ref, kvw_ref, heads_q, total, kept, gain, lost, tri, gathered, mixers,
    arrive, spare_arrive, up_sem, side_sem, over_sem, own_sem, mix_send, mix_arrive, mix_local, att_send, att_arrive, load_sem,
):
    rows = hidden_ref.shape[0]
    heads = kv_count * share
    kv_width = kv_count * HEAD_DIM
    me = lax.axis_index("sp")
    rank = lax.axis_index("tp")
    levels = devices // PLANE
    level = me // PLANE
    place = me % PLANE
    across = PLANE - 1 - place
    side = place + 1 - 2 * (place % 2)
    over = (place + 2) % PLANE
    has_up = level < levels - 1
    offset = me * rows

    def slot(block):
        return pairs.at[pl.ds(pl.multiple_of(block * rows, 16), rows), :]

    def ship(source, block, send, target):
        return pltpu.make_async_remote_copy(
            src_ref=source, dst_ref=slot(block), send_sem=send, recv_sem=arrive.at[block],
            device_id={"sp": target}, device_id_type=MESH,
        )

    def own_to(index, where):
        return ship(kv_ref, me, own_sem.at[index], level * PLANE + where)

    def own_spare():
        return pltpu.make_async_remote_copy(
            src_ref=kv_ref, dst_ref=spare, send_sem=own_sem.at[2], recv_sem=spare_arrive,
            device_id={"sp": level * PLANE + across}, device_id_type=MESH,
        )

    def lift_up():
        return ship(spare, level * PLANE + across, up_sem.at[level * PLANE + across], me + PLANE)

    def own_up():
        return ship(kv_ref, me, up_sem.at[me], me + PLANE)

    def send_up(block):
        return ship(slot(block), block, up_sem.at[block], me + PLANE)

    def send_side(block):
        return ship(slot(block), block, side_sem.at[block], level * PLANE + side)

    def send_over(block):
        return ship(slot(block), block, over_sem.at[block], level * PLANE + over)

    def mixer(step):
        return pltpu.make_async_remote_copy(
            src_ref=mix_ref, dst_ref=mixers.at[rank], send_sem=mix_send.at[step],
            recv_sem=mix_arrive.at[step], device_id={"tp": (rank + step) % ranks}, device_id_type=MESH,
        )

    def attended(step):
        return pltpu.make_async_remote_copy(
            src_ref=gathered.at[rank], dst_ref=gathered.at[rank], send_sem=att_send.at[step],
            recv_sem=att_arrive.at[step], device_id={"tp": (rank + step) % ranks}, device_id_type=MESH,
        )

    if sliced:
        column = pl.multiple_of(rank * kv_width, kv_width)
        loads = [
            pltpu.make_async_copy(
                source.at[:, pl.ds(column, kv_width)],
                kvw_ref.at[:, pl.ds(index * kv_width, kv_width)],
                load_sem.at[index],
            )
            for index, source in enumerate((kw_hbm, vw_hbm))
        ]
    else:
        loads = [pltpu.make_async_copy(kw_hbm, kvw_ref, load_sem.at[0])]
    query_load = pltpu.make_async_copy(qw_hbm, qw_ref, load_sem.at[2])
    for load in loads:
        load.start()
    query_load.start()

    barrier = pltpu.get_barrier_semaphore()

    def greet(**where):
        pl.semaphore_signal(barrier, inc=1, device_id=where, device_id_type=MESH)

    for where in (side, over, across):
        greet(sp=level * PLANE + where)
    for step in range(1, ranks):
        greet(tp=(rank + step) % ranks)
    pl.when(has_up)(lambda: greet(sp=me + PLANE))
    pl.when(level > 0)(lambda: greet(sp=me - PLANE))
    wide = hidden_ref[...].astype(jnp.float32)
    normed = wide * lax.rsqrt(jnp.mean(wide * wide, axis=-1, keepdims=True) + 1e-06) * gain_ref[...]
    normed_ref[...] = normed.astype(jnp.bfloat16)
    for load in loads:
        load.wait()
    key_value = jnp.dot(normed_ref[...], kvw_ref[...], preferred_element_type=jnp.float32)
    key_value = key_value.astype(jnp.bfloat16)
    kv_ref[...] = key_value
    pairs[pl.ds(pl.multiple_of(offset, 16), rows), :] = key_value
    pl.semaphore_wait(
        barrier, 2 + ranks + jnp.minimum(level, 1) + jnp.minimum(levels - 1 - level, 1)
    )

    pl.when(has_up)(lambda: own_up().start())
    pl.when((across > place) & has_up)(lambda: own_to(2, across).start())
    pl.when((across < place) & has_up)(lambda: own_spare().start())
    pl.when(side > place)(lambda: own_to(0, side).start())
    pl.when(over > place)(lambda: own_to(1, over).start())
    pl.when((across > place) & (level == levels - 1))(lambda: own_to(2, across).start())
    mine = pltpu.make_async_copy(mix_ref, mixers.at[rank], mix_local)
    mine.start()
    for step in range(1, ranks):
        mixer(step).start()

    query_load.wait()
    queries = jnp.dot(normed_ref[...], qw_ref[...], preferred_element_type=jnp.float32)
    queries = queries.astype(jnp.bfloat16)
    for h in range(heads):
        heads_q[h] = queries[:, h * HEAD_DIM : (h + 1) * HEAD_DIM]
    total[...] = jnp.zeros_like(total)
    kept[...] = jnp.zeros_like(kept)
    first_pos = lax.broadcasted_iota(jnp.int32, (span, span), 0)
    second_pos = lax.broadcasted_iota(jnp.int32, (span, span), 1)
    tri[...] = (first_pos > second_pos).astype(jnp.float32).astype(jnp.bfloat16)

    def arrived(block):
        ship(slot(block), block, up_sem.at[block], (me + 1) % devices).wait_recv()

    def relay_column(block):
        arrived(block)
        pl.when(has_up)(lambda: send_up(block).start())
        send_side(block).start()
        send_over(block).start()

    def relay_across(block):
        arrived(block)
        pl.when(has_up)(lambda: send_up(block).start())

    def lift():
        own_spare().wait_recv()
        lift_up().start()

    def relay(group):
        lower = level - group
        held = lower * PLANE + across
        pl.when(lower >= 1)(lambda: relay_column((lower - 1) * PLANE + place))
        pl.when((group == 0) & has_up & (across > place))(lift)
        pl.when((group > 0) | ((across < place) & has_up))(lambda: relay_across(held))

    def relay_until(done, count):
        count = jnp.minimum(count, level + 1)
        ahead = jnp.maximum(count - done, 0)

        def one(index, _):
            relay(done + index)
            return 0

        lax.fori_loop(0, ahead, one, 0)
        return done + ahead

    def take_until(front, low):
        count = jnp.maximum(front - low, 0)

        def one(index, _):
            block = front - 1 - index
            spot = block % PLANE
            near = (block // PLANE == level) & (level == levels - 1)
            pl.when((spot != place) & ((spot != across) | near))(lambda: arrived(block))
            return 0

        lax.fori_loop(0, count, one, 0)
        return front - count

    def advance(state, start, turn):
        done, front = state
        low = start // rows
        done = relay_until(done, jnp.maximum(turn // PACE + 1, level - low // PLANE + 1))
        return done, take_until(front, low)

    def chunk(start, masked):
        start = pl.multiple_of(start, span)
        block = pairs[pl.ds(start, span), :]
        if masked:
            key_pos = start + lax.broadcasted_iota(jnp.int32, (rows, span), 1)
            query_pos = offset + lax.broadcasted_iota(jnp.int32, (rows, span), 0)
            strict = key_pos < query_pos
            value_pos = start + lax.broadcasted_iota(jnp.int32, (span, block.shape[1]), 0)
            block = jnp.where(value_pos < offset + rows, block.astype(jnp.float32), 0.0)
            block = block.astype(jnp.bfloat16)
        later = tri[...]
        scale = HEAD_DIM ** (-0.5) * LOG2E
        tiles = [(h, t) for h in range(heads) for t in range(0, rows, ROWS)]

        def first(h, t):
            g = h // share
            dots = lax.dot_general(
                heads_q[h, t : t + ROWS], block[:, g * HEAD_DIM : (g + 1) * HEAD_DIM],
                (((1,), (1,)), ((), ())), preferred_element_type=jnp.float32,
            )
            u = dots * scale + bias_ref[h] * LOG2E
            drop = jnp.maximum(u, jnp.log2(1.0 + jnp.exp2(jnp.minimum(u, 126.0))))
            if masked:
                drop = jnp.where(strict[t : t + ROWS], drop, 0.0)
            gain[h, t : t + ROWS] = u - drop
            lost[h, t : t + ROWS] = drop.astype(jnp.bfloat16)
            return drop[:, :1]

        def second(h, t, head):
            g = h // share
            part = slice(t, t + ROWS)
            after = jnp.dot(lost[h, part], later, preferred_element_type=jnp.float32)
            weight = jnp.exp2(gain[h, part] - (after + jnp.tile(kept[h, part], (1, span // 128))))
            if masked:
                weight = jnp.where(strict[part], weight, 0.0)
            kept[h, part] += jnp.broadcast_to(after[:, :1] + head, (ROWS, 128))
            total[h, part] += jnp.dot(
                weight.astype(jnp.bfloat16),
                block[:, kv_width + g * HEAD_DIM : kv_width + (g + 1) * HEAD_DIM],
                preferred_element_type=jnp.float32,
            )

        waiting = []
        for h, t in tiles:
            waiting.append((h, t, first(h, t)))
            if len(waiting) > LAG:
                second(*waiting.pop(0))
        for item in waiting:
            second(*item)

    whole = offset // span
    turns = (offset + rows + span - 1) // span

    def edge(turn, state):
        start = (turns - 1 - turn) * span
        state = advance(state, start, turn)
        chunk(start, True)
        return state

    def plain(turn, state):
        start = (whole - 1 - turn) * span
        state = advance(state, start, turn + turns - whole)
        chunk(start, False)
        return state

    state = lax.fori_loop(0, turns - whole, edge, (0, me))
    done, front = lax.fori_loop(0, whole, plain, state)
    relay_until(done, level + 1)
    take_until(front, 0)

    for h in range(heads):
        gathered[rank, :, h * HEAD_DIM : (h + 1) * HEAD_DIM] = total[h].astype(jnp.bfloat16)
    for step in range(1, ranks):
        attended(step).start()
    mine.wait()
    for step in range(1, ranks):
        mixer(step).wait_recv()
    for step in range(1, ranks):
        attended(step).wait_recv()
    features = out_ref.shape[1]
    tile = math.gcd(features, 512)
    for column in range(0, features, tile):
        summed = jnp.zeros((rows, tile), jnp.float32)
        for r in range(ranks):
            summed += jnp.dot(
                gathered[r], mixers[r, :, column : column + tile], preferred_element_type=jnp.float32
            )
        out_ref[:, column : column + tile] = summed.astype(jnp.bfloat16)

    pl.when(side > place)(lambda: own_to(0, side).wait_send())
    pl.when(over > place)(lambda: own_to(1, over).wait_send())
    pl.when(across > place)(lambda: own_to(2, across).wait_send())
    pl.when((across < place) & has_up)(lambda: own_spare().wait_send())
    pl.when(has_up)(lambda: own_up().wait_send())
    pl.when(has_up & (across > place))(lambda: lift_up().wait_send())

    def settle(block, _):
        spot = block % PLANE
        lower = block // PLANE < level

        def plane_done():
            send_side(block).wait_send()
            send_over(block).wait_send()

        pl.when(has_up & ((spot == place) | (spot == across)))(lambda: send_up(block).wait_send())
        pl.when(lower & (spot == place))(plane_done)
        return 0

    lax.fori_loop(0, me, settle, 0)
    for step in range(1, ranks):
        mixer(step).wait_send()
        attended(step).wait_send()


def local(hidden, norm_gain, query_weight, key_weight, value_weight, head_bias, output_weight):
    group = HEADS // KV_HEADS
    local_heads = query_weight.shape[1] // HEAD_DIM
    kv_count = max(1, local_heads // group)
    share = min(local_heads, group)
    kv_width = kv_count * HEAD_DIM
    sliced = kv_width % 128 == 0 and local_heads % group == 0
    if sliced:
        key_side, value_side = key_weight, value_weight
    else:
        first = lax.axis_index("tp") * local_heads // group
        key_cols = lax.dynamic_slice_in_dim(key_weight, first * HEAD_DIM, kv_width, 1)
        value_cols = lax.dynamic_slice_in_dim(value_weight, first * HEAD_DIM, kv_width, 1)
        key_side = value_side = jnp.concatenate([key_cols, value_cols], axis=1)
    rows = hidden.shape[0]
    devices = lax.axis_size("sp")
    ranks = lax.axis_size("tp")
    span = math.gcd(rows * devices, 256)
    width = query_weight.shape[1]
    features = output_weight.shape[1]
    vmem = pl.BlockSpec(memory_space=pltpu.VMEM)
    hbm = pl.BlockSpec(memory_space=pl.ANY)
    dma = pltpu.SemaphoreType.DMA
    return pl.pallas_call(
        functools.partial(layer_kernel, span, kv_count, share, devices, ranks, sliced),
        out_shape=jax.ShapeDtypeStruct((rows, features), jnp.bfloat16),
        in_specs=[
            pl.BlockSpec(memory_space=pltpu.SMEM),
            vmem,
            vmem,
            hbm,
            hbm,
            hbm,
            hbm,
        ],
        out_specs=vmem,
        scratch_shapes=[
            pltpu.VMEM((rows * devices, 2 * kv_width), jnp.bfloat16),
            pltpu.VMEM((rows, 2 * kv_width), jnp.bfloat16),
            pltpu.VMEM(hidden.shape, jnp.bfloat16),
            pltpu.VMEM((rows, 2 * kv_width), jnp.bfloat16),
            pltpu.VMEM(query_weight.shape, jnp.bfloat16),
            pltpu.VMEM((query_weight.shape[0], 2 * kv_width), jnp.bfloat16),
            pltpu.VMEM((local_heads, rows, HEAD_DIM), jnp.bfloat16),
            pltpu.VMEM((local_heads, rows, HEAD_DIM), jnp.float32),
            pltpu.VMEM((local_heads, rows, 128), jnp.float32),
            pltpu.VMEM((local_heads, rows, span), jnp.float32),
            pltpu.VMEM((local_heads, rows, span), jnp.bfloat16),
            pltpu.VMEM((span, span), jnp.bfloat16),
            pltpu.VMEM((ranks, rows, width), jnp.bfloat16),
            pltpu.VMEM((ranks, width, features), jnp.bfloat16),
            dma((devices,)),
            dma,
            dma((devices,)),
            dma((devices,)),
            dma((devices,)),
            dma((3,)),
            dma((ranks,)),
            dma((ranks,)),
            dma,
            dma((ranks,)),
            dma((ranks,)),
            dma((3,)),
        ],
        compiler_params=pltpu.CompilerParams(has_side_effects=True, collective_id=0),
    )(head_bias, hidden, norm_gain[None, :], query_weight, key_side, value_side, output_weight)


def solution(mesh):
    placed = (P("sp", None), P(), P(None, "tp"), P(), P(), P("tp"), P("tp", None))
    return jax.shard_map(
        local, mesh=mesh, in_specs=placed, out_specs=P("sp", None), check_vma=False
    )
```

```python
import functools
import math

import jax
import jax.numpy as jnp
from jax import lax
from jax.experimental import pallas as pl
from jax.experimental.pallas import tpu as pltpu
from jax.sharding import PartitionSpec as P

HEADS = 16
KV_HEADS = 4
HEAD_DIM = 64
LOG2E = math.log2(math.e)


PLANE = 4
PACE = 3
ROWS = 192
LAG = 8
MESH = pl.DeviceIdType.MESH


def layer_kernel(
    span, kv_count, share, devices, ranks, sliced,
    bias_ref, hidden_ref, gain_ref, qw_hbm, kw_hbm, vw_hbm, mix_ref, out_ref,
    pairs, spare, normed_ref, kv_ref, qw_ref, kvw_ref, heads_q, total, kept, gain, lost, tri, gathered, mixers,
    arrive, spare_arrive, up_sem, side_sem, over_sem, own_sem, mix_send, mix_arrive, mix_local, att_send, att_arrive, load_sem,
):
    rows = hidden_ref.shape[0]
    heads = kv_count * share
    kv_width = kv_count * HEAD_DIM
    me = lax.axis_index("sp")
    rank = lax.axis_index("tp")
    levels = devices // PLANE
    level = me // PLANE
    place = me % PLANE
    across = PLANE - 1 - place
    side = place + 1 - 2 * (place % 2)
    over = (place + 2) % PLANE
    has_up = level < levels - 1
    offset = me * rows

    def slot(block):
        return pairs.at[pl.ds(pl.multiple_of(block * rows, 16), rows), :]

    def ship(source, block, send, target):
        return pltpu.make_async_remote_copy(
            src_ref=source, dst_ref=slot(block), send_sem=send, recv_sem=arrive.at[block],
            device_id={"sp": target}, device_id_type=MESH,
        )

    def own_to(index, where):
        return ship(kv_ref, me, own_sem.at[index], level * PLANE + where)

    def own_spare():
        return pltpu.make_async_remote_copy(
            src_ref=kv_ref, dst_ref=spare, send_sem=own_sem.at[2], recv_sem=spare_arrive,
            device_id={"sp": level * PLANE + across}, device_id_type=MESH,
        )

    def lift_up():
        return ship(spare, level * PLANE + across, up_sem.at[level * PLANE + across], me + PLANE)

    def own_up():
        return ship(kv_ref, me, up_sem.at[me], me + PLANE)

    def send_up(block):
        return ship(slot(block), block, up_sem.at[block], me + PLANE)

    def send_side(block):
        return ship(slot(block), block, side_sem.at[block], level * PLANE + side)

    def send_over(block):
        return ship(slot(block), block, over_sem.at[block], level * PLANE + over)

    def mixer(step):
        return pltpu.make_async_remote_copy(
            src_ref=mix_ref, dst_ref=mixers.at[rank], send_sem=mix_send.at[step],
            recv_sem=mix_arrive.at[step], device_id={"tp": (rank + step) % ranks}, device_id_type=MESH,
        )

    def attended(step):
        return pltpu.make_async_remote_copy(
            src_ref=gathered.at[rank], dst_ref=gathered.at[rank], send_sem=att_send.at[step],
            recv_sem=att_arrive.at[step], device_id={"tp": (rank + step) % ranks}, device_id_type=MESH,
        )

    if sliced:
        column = pl.multiple_of(rank * kv_width, kv_width)
        loads = [
            pltpu.make_async_copy(
                source.at[:, pl.ds(column, kv_width)],
                kvw_ref.at[:, pl.ds(index * kv_width, kv_width)],
                load_sem.at[index],
            )
            for index, source in enumerate((kw_hbm, vw_hbm))
        ]
    else:
        loads = [pltpu.make_async_copy(kw_hbm, kvw_ref, load_sem.at[0])]
    query_load = pltpu.make_async_copy(qw_hbm, qw_ref, load_sem.at[2])
    for load in loads:
        load.start()
    query_load.start()

    barrier = pltpu.get_barrier_semaphore()

    def greet(**where):
        pl.semaphore_signal(barrier, inc=1, device_id=where, device_id_type=MESH)

    for where in (side, over, across):
        greet(sp=level * PLANE + where)
    for step in range(1, ranks):
        greet(tp=(rank + step) % ranks)
    pl.when(has_up)(lambda: greet(sp=me + PLANE))
    pl.when(level > 0)(lambda: greet(sp=me - PLANE))
    wide = hidden_ref[...].astype(jnp.float32)
    normed = wide * lax.rsqrt(jnp.mean(wide * wide, axis=-1, keepdims=True) + 1e-06) * gain_ref[...]
    normed_ref[...] = normed.astype(jnp.bfloat16)
    for load in loads:
        load.wait()
    key_value = jnp.dot(normed_ref[...], kvw_ref[...], preferred_element_type=jnp.float32)
    key_value = key_value.astype(jnp.bfloat16)
    kv_ref[...] = key_value
    pairs[pl.ds(pl.multiple_of(offset, 16), rows), :] = key_value
    pl.semaphore_wait(
        barrier, 2 + ranks + jnp.minimum(level, 1) + jnp.minimum(levels - 1 - level, 1)
    )

    pl.when(has_up)(lambda: own_up().start())
    pl.when((across > place) & has_up)(lambda: own_to(2, across).start())
    pl.when((across < place) & has_up)(lambda: own_spare().start())
    pl.when(side > place)(lambda: own_to(0, side).start())
    pl.when(over > place)(lambda: own_to(1, over).start())
    pl.when((across > place) & (level == levels - 1))(lambda: own_to(2, across).start())
    mine = pltpu.make_async_copy(mix_ref, mixers.at[rank], mix_local)
    mine.start()
    for step in range(1, ranks):
        mixer(step).start()

    query_load.wait()
    queries = jnp.dot(normed_ref[...], qw_ref[...], preferred_element_type=jnp.float32)
    queries = queries.astype(jnp.bfloat16)
    for h in range(heads):
        heads_q[h] = queries[:, h * HEAD_DIM : (h + 1) * HEAD_DIM]
    total[...] = jnp.zeros_like(total)
    kept[...] = jnp.zeros_like(kept)
    first_pos = lax.broadcasted_iota(jnp.int32, (span, span), 0)
    second_pos = lax.broadcasted_iota(jnp.int32, (span, span), 1)
    tri[...] = (first_pos > second_pos).astype(jnp.float32).astype(jnp.bfloat16)

    def arrived(block):
        ship(slot(block), block, up_sem.at[block], (me + 1) % devices).wait_recv()

    def relay_column(block):
        arrived(block)
        pl.when(has_up)(lambda: send_up(block).start())
        send_side(block).start()
        send_over(block).start()

    def relay_across(block):
        arrived(block)
        pl.when(has_up)(lambda: send_up(block).start())

    def lift():
        own_spare().wait_recv()
        lift_up().start()

    def relay(group):
        lower = level - group
        held = lower * PLANE + across
        pl.when(lower >= 1)(lambda: relay_column((lower - 1) * PLANE + place))
        pl.when((group == 0) & has_up & (across > place))(lift)
        pl.when((group > 0) | ((across < place) & has_up))(lambda: relay_across(held))

    def relay_until(done, count):
        count = jnp.minimum(count, level + 1)
        ahead = jnp.maximum(count - done, 0)

        def one(index, _):
            relay(done + index)
            return 0

        lax.fori_loop(0, ahead, one, 0)
        return done + ahead

    def take_until(front, low):
        count = jnp.maximum(front - low, 0)

        def one(index, _):
            block = front - 1 - index
            spot = block % PLANE
            near = (block // PLANE == level) & (level == levels - 1)
            pl.when((spot != place) & ((spot != across) | near))(lambda: arrived(block))
            return 0

        lax.fori_loop(0, count, one, 0)
        return front - count

    def advance(state, start, turn):
        done, front = state
        low = start // rows
        done = relay_until(done, jnp.maximum(turn // PACE + 1, level - low // PLANE + 1))
        return done, take_until(front, low)

    def chunk(start, masked):
        start = pl.multiple_of(start, span)
        block = pairs[pl.ds(start, span), :]
        if masked:
            key_pos = start + lax.broadcasted_iota(jnp.int32, (rows, span), 1)
            query_pos = offset + lax.broadcasted_iota(jnp.int32, (rows, span), 0)
            strict = key_pos < query_pos
            value_pos = start + lax.broadcasted_iota(jnp.int32, (span, block.shape[1]), 0)
            block = jnp.where(value_pos < offset + rows, block.astype(jnp.float32), 0.0)
            block = block.astype(jnp.bfloat16)
        later = tri[...]
        scale = HEAD_DIM ** (-0.5) * LOG2E
        tiles = [(h, t) for h in range(heads) for t in range(0, rows, ROWS)]

        def first(h, t):
            g = h // share
            dots = lax.dot_general(
                heads_q[h, t : t + ROWS], block[:, g * HEAD_DIM : (g + 1) * HEAD_DIM],
                (((1,), (1,)), ((), ())), preferred_element_type=jnp.float32,
            )
            u = dots * scale + bias_ref[h] * LOG2E
            drop = jnp.maximum(u, jnp.log2(1.0 + jnp.exp2(jnp.minimum(u, 126.0))))
            if masked:
                drop = jnp.where(strict[t : t + ROWS], drop, 0.0)
            gain[h, t : t + ROWS] = u - drop
            lost[h, t : t + ROWS] = drop.astype(jnp.bfloat16)
            return drop[:, :1]

        def second(h, t, head):
            part = slice(t, t + ROWS)
            after = jnp.dot(lost[h, part], later, preferred_element_type=jnp.float32)
            weight = jnp.exp2(gain[h, part] - (after + jnp.tile(kept[h, part], (1, span // 128))))
            if masked:
                weight = jnp.where(strict[part], weight, 0.0)
            kept[h, part] += jnp.broadcast_to(after[:, :1] + head, (ROWS, 128))
            lost[h, part] = weight.astype(jnp.bfloat16)

        def third(h, t):
            g = h // share
            part = slice(t, t + ROWS)
            total[h, part] += jnp.dot(
                lost[h, part],
                block[:, kv_width + g * HEAD_DIM : kv_width + (g + 1) * HEAD_DIM],
                preferred_element_type=jnp.float32,
            )

        waiting = []
        for h, t in tiles:
            waiting.append((h, t, first(h, t)))
            if len(waiting) > LAG:
                second(*waiting.pop(0))
        for item in waiting:
            second(*item)
        for h, t in tiles:
            third(h, t)

    whole = offset // span
    turns = (offset + rows + span - 1) // span

    def edge(turn, state):
        start = (turns - 1 - turn) * span
        state = advance(state, start, turn)
        chunk(start, True)
        return state

    def plain(turn, state):
        start = (whole - 1 - turn) * span
        state = advance(state, start, turn + turns - whole)
        chunk(start, False)
        return state

    state = lax.fori_loop(0, turns - whole, edge, (0, me))
    done, front = lax.fori_loop(0, whole, plain, state)
    relay_until(done, level + 1)
    take_until(front, 0)

    for h in range(heads):
        gathered[rank, :, h * HEAD_DIM : (h + 1) * HEAD_DIM] = total[h].astype(jnp.bfloat16)
    for step in range(1, ranks):
        attended(step).start()
    mine.wait()
    for step in range(1, ranks):
        mixer(step).wait_recv()
    for step in range(1, ranks):
        attended(step).wait_recv()
    features = out_ref.shape[1]
    tile = math.gcd(features, 512)
    for column in range(0, features, tile):
        summed = jnp.zeros((rows, tile), jnp.float32)
        for r in range(ranks):
            summed += jnp.dot(
                gathered[r], mixers[r, :, column : column + tile], preferred_element_type=jnp.float32
            )
        out_ref[:, column : column + tile] = summed.astype(jnp.bfloat16)

    pl.when(side > place)(lambda: own_to(0, side).wait_send())
    pl.when(over > place)(lambda: own_to(1, over).wait_send())
    pl.when(across > place)(lambda: own_to(2, across).wait_send())
    pl.when((across < place) & has_up)(lambda: own_spare().wait_send())
    pl.when(has_up)(lambda: own_up().wait_send())
    pl.when(has_up & (across > place))(lambda: lift_up().wait_send())

    def settle(block, _):
        spot = block % PLANE
        lower = block // PLANE < level

        def plane_done():
            send_side(block).wait_send()
            send_over(block).wait_send()

        pl.when(has_up & ((spot == place) | (spot == across)))(lambda: send_up(block).wait_send())
        pl.when(lower & (spot == place))(plane_done)
        return 0

    lax.fori_loop(0, me, settle, 0)
    for step in range(1, ranks):
        mixer(step).wait_send()
        attended(step).wait_send()


def local(hidden, norm_gain, query_weight, key_weight, value_weight, head_bias, output_weight):
    group = HEADS // KV_HEADS
    local_heads = query_weight.shape[1] // HEAD_DIM
    kv_count = max(1, local_heads // group)
    share = min(local_heads, group)
    kv_width = kv_count * HEAD_DIM
    sliced = kv_width % 128 == 0 and local_heads % group == 0
    if sliced:
        key_side, value_side = key_weight, value_weight
    else:
        first = lax.axis_index("tp") * local_heads // group
        key_cols = lax.dynamic_slice_in_dim(key_weight, first * HEAD_DIM, kv_width, 1)
        value_cols = lax.dynamic_slice_in_dim(value_weight, first * HEAD_DIM, kv_width, 1)
        key_side = value_side = jnp.concatenate([key_cols, value_cols], axis=1)
    rows = hidden.shape[0]
    devices = lax.axis_size("sp")
    ranks = lax.axis_size("tp")
    span = math.gcd(rows * devices, 256)
    width = query_weight.shape[1]
    features = output_weight.shape[1]
    vmem = pl.BlockSpec(memory_space=pltpu.VMEM)
    hbm = pl.BlockSpec(memory_space=pl.ANY)
    dma = pltpu.SemaphoreType.DMA
    return pl.pallas_call(
        functools.partial(layer_kernel, span, kv_count, share, devices, ranks, sliced),
        out_shape=jax.ShapeDtypeStruct((rows, features), jnp.bfloat16),
        in_specs=[
            pl.BlockSpec(memory_space=pltpu.SMEM),
            vmem,
            vmem,
            hbm,
            hbm,
            hbm,
            hbm,
        ],
        out_specs=vmem,
        scratch_shapes=[
            pltpu.VMEM((rows * devices, 2 * kv_width), jnp.bfloat16),
            pltpu.VMEM((rows, 2 * kv_width), jnp.bfloat16),
            pltpu.VMEM(hidden.shape, jnp.bfloat16),
            pltpu.VMEM((rows, 2 * kv_width), jnp.bfloat16),
            pltpu.VMEM(query_weight.shape, jnp.bfloat16),
            pltpu.VMEM((query_weight.shape[0], 2 * kv_width), jnp.bfloat16),
            pltpu.VMEM((local_heads, rows, HEAD_DIM), jnp.bfloat16),
            pltpu.VMEM((local_heads, rows, HEAD_DIM), jnp.float32),
            pltpu.VMEM((local_heads, rows, 128), jnp.float32),
            pltpu.VMEM((local_heads, rows, span), jnp.float32),
            pltpu.VMEM((local_heads, rows, span), jnp.bfloat16),
            pltpu.VMEM((span, span), jnp.bfloat16),
            pltpu.VMEM((ranks, rows, width), jnp.bfloat16),
            pltpu.VMEM((ranks, width, features), jnp.bfloat16),
            dma((devices,)),
            dma,
            dma((devices,)),
            dma((devices,)),
            dma((devices,)),
            dma((3,)),
            dma((ranks,)),
            dma((ranks,)),
            dma,
            dma((ranks,)),
            dma((ranks,)),
            dma((3,)),
        ],
        compiler_params=pltpu.CompilerParams(has_side_effects=True, collective_id=0),
    )(head_bias, hidden, norm_gain[None, :], query_weight, key_side, value_side, output_weight)


def solution(mesh):
    placed = (P("sp", None), P(), P(None, "tp"), P(), P(), P("tp"), P("tp", None))
    return jax.shard_map(
        local, mesh=mesh, in_specs=placed, out_specs=P("sp", None), check_vma=False
    )
```

```python
import functools
import math

import jax
import jax.numpy as jnp
from jax import lax
from jax.experimental import pallas as pl
from jax.experimental.pallas import tpu as pltpu
from jax.sharding import PartitionSpec as P

HEADS = 16
KV_HEADS = 4
HEAD_DIM = 64
LOG2E = math.log2(math.e)


PLANE = 4
PACE = 4
ROWS = 192
LAG = 8
MESH = pl.DeviceIdType.MESH


def layer_kernel(
    span, kv_count, share, devices, ranks, sliced,
    bias_ref, hidden_ref, gain_ref, qw_hbm, kw_hbm, vw_hbm, mix_ref, out_ref,
    pairs, spare, normed_ref, kv_ref, qw_ref, kvw_ref, heads_q, total, kept, gain, lost, tri, gathered, mixers,
    arrive, spare_arrive, up_sem, side_sem, over_sem, own_sem, mix_send, mix_arrive, mix_local, att_send, att_arrive, load_sem,
):
    rows = hidden_ref.shape[0]
    heads = kv_count * share
    kv_width = kv_count * HEAD_DIM
    me = lax.axis_index("sp")
    rank = lax.axis_index("tp")
    levels = devices // PLANE
    level = me // PLANE
    place = me % PLANE
    across = PLANE - 1 - place
    side = place + 1 - 2 * (place % 2)
    over = (place + 2) % PLANE
    has_up = level < levels - 1
    offset = me * rows

    def slot(block):
        return pairs.at[pl.ds(pl.multiple_of(block * rows, 16), rows), :]

    def ship(source, block, send, target):
        return pltpu.make_async_remote_copy(
            src_ref=source, dst_ref=slot(block), send_sem=send, recv_sem=arrive.at[block],
            device_id={"sp": target}, device_id_type=MESH,
        )

    def own_to(index, where):
        return ship(kv_ref, me, own_sem.at[index], level * PLANE + where)

    def own_spare():
        return pltpu.make_async_remote_copy(
            src_ref=kv_ref, dst_ref=spare, send_sem=own_sem.at[2], recv_sem=spare_arrive,
            device_id={"sp": level * PLANE + across}, device_id_type=MESH,
        )

    def lift_up():
        return ship(spare, level * PLANE + across, up_sem.at[level * PLANE + across], me + PLANE)

    def own_up():
        return ship(kv_ref, me, up_sem.at[me], me + PLANE)

    def send_up(block):
        return ship(slot(block), block, up_sem.at[block], me + PLANE)

    def send_side(block):
        return ship(slot(block), block, side_sem.at[block], level * PLANE + side)

    def send_over(block):
        return ship(slot(block), block, over_sem.at[block], level * PLANE + over)

    def mixer(step):
        return pltpu.make_async_remote_copy(
            src_ref=mix_ref, dst_ref=mixers.at[rank], send_sem=mix_send.at[step],
            recv_sem=mix_arrive.at[step], device_id={"tp": (rank + step) % ranks}, device_id_type=MESH,
        )

    def attended(step):
        return pltpu.make_async_remote_copy(
            src_ref=gathered.at[rank], dst_ref=gathered.at[rank], send_sem=att_send.at[step],
            recv_sem=att_arrive.at[step], device_id={"tp": (rank + step) % ranks}, device_id_type=MESH,
        )

    if sliced:
        column = pl.multiple_of(rank * kv_width, kv_width)
        loads = [
            pltpu.make_async_copy(
                source.at[:, pl.ds(column, kv_width)],
                kvw_ref.at[:, pl.ds(index * kv_width, kv_width)],
                load_sem.at[index],
            )
            for index, source in enumerate((kw_hbm, vw_hbm))
        ]
    else:
        loads = [pltpu.make_async_copy(kw_hbm, kvw_ref, load_sem.at[0])]
    query_load = pltpu.make_async_copy(qw_hbm, qw_ref, load_sem.at[2])
    for load in loads:
        load.start()
    query_load.start()

    barrier = pltpu.get_barrier_semaphore()

    def greet(**where):
        pl.semaphore_signal(barrier, inc=1, device_id=where, device_id_type=MESH)

    for where in (side, over, across):
        greet(sp=level * PLANE + where)
    for step in range(1, ranks):
        greet(tp=(rank + step) % ranks)
    pl.when(has_up)(lambda: greet(sp=me + PLANE))
    pl.when(level > 0)(lambda: greet(sp=me - PLANE))
    wide = hidden_ref[...].astype(jnp.float32)
    normed = wide * lax.rsqrt(jnp.mean(wide * wide, axis=-1, keepdims=True) + 1e-06) * gain_ref[...]
    normed_ref[...] = normed.astype(jnp.bfloat16)
    for load in loads:
        load.wait()
    key_value = jnp.dot(normed_ref[...], kvw_ref[...], preferred_element_type=jnp.float32)
    key_value = key_value.astype(jnp.bfloat16)
    kv_ref[...] = key_value
    pairs[pl.ds(pl.multiple_of(offset, 16), rows), :] = key_value
    pl.semaphore_wait(
        barrier, 2 + ranks + jnp.minimum(level, 1) + jnp.minimum(levels - 1 - level, 1)
    )

    pl.when(has_up)(lambda: own_up().start())
    pl.when((across > place) & has_up)(lambda: own_to(2, across).start())
    pl.when((across < place) & has_up)(lambda: own_spare().start())
    pl.when(side > place)(lambda: own_to(0, side).start())
    pl.when(over > place)(lambda: own_to(1, over).start())
    pl.when((across > place) & (level == levels - 1))(lambda: own_to(2, across).start())
    mine = pltpu.make_async_copy(mix_ref, mixers.at[rank], mix_local)
    mine.start()
    for step in range(1, ranks):
        mixer(step).start()

    query_load.wait()
    queries = jnp.dot(normed_ref[...], qw_ref[...], preferred_element_type=jnp.float32)
    queries = queries.astype(jnp.bfloat16)
    for h in range(heads):
        heads_q[h] = queries[:, h * HEAD_DIM : (h + 1) * HEAD_DIM]
    total[...] = jnp.zeros_like(total)
    kept[...] = jnp.zeros_like(kept)
    first_pos = lax.broadcasted_iota(jnp.int32, (span, span), 0)
    second_pos = lax.broadcasted_iota(jnp.int32, (span, span), 1)
    tri[...] = (first_pos > second_pos).astype(jnp.float32).astype(jnp.bfloat16)

    def arrived(block):
        ship(slot(block), block, up_sem.at[block], (me + 1) % devices).wait_recv()

    def relay_column(block):
        arrived(block)
        pl.when(has_up)(lambda: send_up(block).start())
        send_side(block).start()
        send_over(block).start()

    def relay_across(block):
        arrived(block)
        pl.when(has_up)(lambda: send_up(block).start())

    def lift():
        own_spare().wait_recv()
        lift_up().start()

    def relay(group):
        lower = level - group
        held = lower * PLANE + across
        pl.when(lower >= 1)(lambda: relay_column((lower - 1) * PLANE + place))
        pl.when((group == 0) & has_up & (across > place))(lift)
        pl.when((group > 0) | ((across < place) & has_up))(lambda: relay_across(held))

    def relay_until(done, count):
        count = jnp.minimum(count, level + 1)
        ahead = jnp.maximum(count - done, 0)

        def one(index, _):
            relay(done + index)
            return 0

        lax.fori_loop(0, ahead, one, 0)
        return done + ahead

    def take_until(front, low):
        count = jnp.maximum(front - low, 0)

        def one(index, _):
            block = front - 1 - index
            spot = block % PLANE
            near = (block // PLANE == level) & (level == levels - 1)
            pl.when((spot != place) & ((spot != across) | near))(lambda: arrived(block))
            return 0

        lax.fori_loop(0, count, one, 0)
        return front - count

    def advance(state, start, turn):
        done, front = state
        low = start // rows
        done = relay_until(done, jnp.maximum(turn // PACE + 1, level - low // PLANE + 1))
        return done, take_until(front, low)

    def chunk(start, masked):
        start = pl.multiple_of(start, span)
        block = pairs[pl.ds(start, span), :]
        if masked:
            key_pos = start + lax.broadcasted_iota(jnp.int32, (rows, span), 1)
            query_pos = offset + lax.broadcasted_iota(jnp.int32, (rows, span), 0)
            strict = key_pos < query_pos
            value_pos = start + lax.broadcasted_iota(jnp.int32, (span, block.shape[1]), 0)
            block = jnp.where(value_pos < offset + rows, block.astype(jnp.float32), 0.0)
            block = block.astype(jnp.bfloat16)
        later = tri[...]
        scale = HEAD_DIM ** (-0.5) * LOG2E
        tiles = [(h, t) for h in range(heads) for t in range(0, rows, ROWS)]

        def first(h, t):
            g = h // share
            dots = lax.dot_general(
                heads_q[h, t : t + ROWS], block[:, g * HEAD_DIM : (g + 1) * HEAD_DIM],
                (((1,), (1,)), ((), ())), preferred_element_type=jnp.float32,
            )
            u = dots * scale + bias_ref[h] * LOG2E
            drop = jnp.maximum(u, jnp.log2(1.0 + jnp.exp2(jnp.minimum(u, 126.0))))
            if masked:
                drop = jnp.where(strict[t : t + ROWS], drop, 0.0)
            gain[h, t : t + ROWS] = u - drop
            lost[h, t : t + ROWS] = drop.astype(jnp.bfloat16)
            return drop[:, :1]

        def second(h, t, head):
            g = h // share
            part = slice(t, t + ROWS)
            after = jnp.dot(lost[h, part], later, preferred_element_type=jnp.float32)
            weight = jnp.exp2(gain[h, part] - (after + jnp.tile(kept[h, part], (1, span // 128))))
            if masked:
                weight = jnp.where(strict[part], weight, 0.0)
            kept[h, part] += jnp.broadcast_to(after[:, :1] + head, (ROWS, 128))
            total[h, part] += jnp.dot(
                weight.astype(jnp.bfloat16),
                block[:, kv_width + g * HEAD_DIM : kv_width + (g + 1) * HEAD_DIM],
                preferred_element_type=jnp.float32,
            )

        waiting = []
        for h, t in tiles:
            waiting.append((h, t, first(h, t)))
            if len(waiting) > LAG:
                second(*waiting.pop(0))
        for item in waiting:
            second(*item)

    whole = offset // span
    turns = (offset + rows + span - 1) // span

    def edge(turn, state):
        start = (turns - 1 - turn) * span
        state = advance(state, start, turn)
        chunk(start, True)
        return state

    def plain(turn, state):
        start = (whole - 1 - turn) * span
        state = advance(state, start, turn + turns - whole)
        chunk(start, False)
        return state

    state = lax.fori_loop(0, turns - whole, edge, (0, me))
    done, front = lax.fori_loop(0, whole, plain, state)
    relay_until(done, level + 1)
    take_until(front, 0)

    for h in range(heads):
        gathered[rank, :, h * HEAD_DIM : (h + 1) * HEAD_DIM] = total[h].astype(jnp.bfloat16)
    for step in range(1, ranks):
        attended(step).start()
    mine.wait()
    for step in range(1, ranks):
        mixer(step).wait_recv()
    for step in range(1, ranks):
        attended(step).wait_recv()
    features = out_ref.shape[1]
    tile = math.gcd(features, 512)
    for column in range(0, features, tile):
        summed = jnp.zeros((rows, tile), jnp.float32)
        for r in range(ranks):
            summed += jnp.dot(
                gathered[r], mixers[r, :, column : column + tile], preferred_element_type=jnp.float32
            )
        out_ref[:, column : column + tile] = summed.astype(jnp.bfloat16)

    pl.when(side > place)(lambda: own_to(0, side).wait_send())
    pl.when(over > place)(lambda: own_to(1, over).wait_send())
    pl.when(across > place)(lambda: own_to(2, across).wait_send())
    pl.when((across < place) & has_up)(lambda: own_spare().wait_send())
    pl.when(has_up)(lambda: own_up().wait_send())
    pl.when(has_up & (across > place))(lambda: lift_up().wait_send())

    def settle(block, _):
        spot = block % PLANE
        lower = block // PLANE < level

        def plane_done():
            send_side(block).wait_send()
            send_over(block).wait_send()

        pl.when(has_up & ((spot == place) | (spot == across)))(lambda: send_up(block).wait_send())
        pl.when(lower & (spot == place))(plane_done)
        return 0

    lax.fori_loop(0, me, settle, 0)
    for step in range(1, ranks):
        mixer(step).wait_send()
        attended(step).wait_send()


def local(hidden, norm_gain, query_weight, key_weight, value_weight, head_bias, output_weight):
    group = HEADS // KV_HEADS
    local_heads = query_weight.shape[1] // HEAD_DIM
    kv_count = max(1, local_heads // group)
    share = min(local_heads, group)
    kv_width = kv_count * HEAD_DIM
    sliced = kv_width % 128 == 0 and local_heads % group == 0
    if sliced:
        key_side, value_side = key_weight, value_weight
    else:
        first = lax.axis_index("tp") * local_heads // group
        key_cols = lax.dynamic_slice_in_dim(key_weight, first * HEAD_DIM, kv_width, 1)
        value_cols = lax.dynamic_slice_in_dim(value_weight, first * HEAD_DIM, kv_width, 1)
        key_side = value_side = jnp.concatenate([key_cols, value_cols], axis=1)
    rows = hidden.shape[0]
    devices = lax.axis_size("sp")
    ranks = lax.axis_size("tp")
    span = math.gcd(rows * devices, 256)
    width = query_weight.shape[1]
    features = output_weight.shape[1]
    vmem = pl.BlockSpec(memory_space=pltpu.VMEM)
    hbm = pl.BlockSpec(memory_space=pl.ANY)
    dma = pltpu.SemaphoreType.DMA
    return pl.pallas_call(
        functools.partial(layer_kernel, span, kv_count, share, devices, ranks, sliced),
        out_shape=jax.ShapeDtypeStruct((rows, features), jnp.bfloat16),
        in_specs=[
            pl.BlockSpec(memory_space=pltpu.SMEM),
            vmem,
            vmem,
            hbm,
            hbm,
            hbm,
            hbm,
        ],
        out_specs=vmem,
        scratch_shapes=[
            pltpu.VMEM((rows * devices, 2 * kv_width), jnp.bfloat16),
            pltpu.VMEM((rows, 2 * kv_width), jnp.bfloat16),
            pltpu.VMEM(hidden.shape, jnp.bfloat16),
            pltpu.VMEM((rows, 2 * kv_width), jnp.bfloat16),
            pltpu.VMEM(query_weight.shape, jnp.bfloat16),
            pltpu.VMEM((query_weight.shape[0], 2 * kv_width), jnp.bfloat16),
            pltpu.VMEM((local_heads, rows, HEAD_DIM), jnp.bfloat16),
            pltpu.VMEM((local_heads, rows, HEAD_DIM), jnp.float32),
            pltpu.VMEM((local_heads, rows, 128), jnp.float32),
            pltpu.VMEM((local_heads, rows, span), jnp.float32),
            pltpu.VMEM((local_heads, rows, span), jnp.bfloat16),
            pltpu.VMEM((span, span), jnp.bfloat16),
            pltpu.VMEM((ranks, rows, width), jnp.bfloat16),
            pltpu.VMEM((ranks, width, features), jnp.bfloat16),
            dma((devices,)),
            dma,
            dma((devices,)),
            dma((devices,)),
            dma((devices,)),
            dma((3,)),
            dma((ranks,)),
            dma((ranks,)),
            dma,
            dma((ranks,)),
            dma((ranks,)),
            dma((3,)),
        ],
        compiler_params=pltpu.CompilerParams(has_side_effects=True, collective_id=0),
    )(head_bias, hidden, norm_gain[None, :], query_weight, key_side, value_side, output_weight)


def solution(mesh):
    placed = (P("sp", None), P(), P(None, "tp"), P(), P(), P("tp"), P("tp", None))
    return jax.shard_map(
        local, mesh=mesh, in_specs=placed, out_specs=P("sp", None), check_vma=False
    )
```
